128 devices in a mesh: ep: 32 (over z, y, core), tp: 4 (over x).
Axes of the slice: x: 4, y: 4, z: 4, core: 2. Of those that a mesh axis runs over, the one named last changes fastest.
Arguments:
- mixer_value: bfloat16 [16384, 2048], P('ep', 'tp'), may hold values from -1 to 2
- mixer_gate: bfloat16 [16384, 2048], P('ep', 'tp'), may hold values from -6 to 6
- mixer_taps: bfloat16 [31, 2048], P(None, 'tp'), may hold values from -60 to 60
- mixer_gain: bfloat16 [2048], P('tp'), may hold values from 0.099609375 to 1.8984375
- mixer_weight: bfloat16 [2048, 4096], P('tp'), may hold values from -0.125 to 0.125
- routed_input: bfloat16 [16384, 4096], P('ep'), may hold values from -6 to 6
- routed_gain: bfloat16 [4096], replicated, may hold values from 0.099609375 to 1.8984375
- expert_ids: int32 [16384, 2], P('ep'), may hold values from 0 to 31, all different within a row; in each aligned block of 128 rows (0 to 127, 128 to 255, ...) at most 10 rows name the same one
- route_share: float32 [16384, 2], P('ep'), may hold values from 0.2 to 1
- gate_weight: bfloat16 [32, 4096, 2048], P('ep', None, 'tp'), may hold values from -0.09375 to 0.09375
- up_weight: bfloat16 [32, 4096, 2048], P('ep', None, 'tp'), may hold values from -0.09375 to 0.09375
- down_weight: bfloat16 [32, 2048, 4096], P('ep', 'tp'), may hold values from -0.125 to 0.125
Outputs:
- mixer_result: bfloat16 [16384, 4096], P(('ep', 'tp'))
- routed_result: bfloat16 [16384, 4096], P(('ep', 'tp'))
The draws below stay inside these ranges and needn't reach their ends.
Inputs may be any that keep to these rules, and one draw needn't show every extreme that they name: `expert_ids`: the two numbers of a row differ. In each aligned block of 128 rows no expert is named by more than 10 rows, and in every draw some expert is named by exactly 10 rows of some block.
All inputs are finite; a program needn't handle non-finite values.
Results may differ from the reference program's by a relative error of at most 0.011.
Values may be sent and summed in bfloat16 or wider, within the bound.
No kernel may reach another device: no remote copies, remote signals or barrier semaphores. Data moves between devices by JAX's collectives and lax.ppermute only.
A program may use at most 192 MiB of HBM per device.

```python
import math
import jax
import jax.numpy as jnp
import numpy as np
from jax import lax

WIDTH = 4096
CHANNELS = 2048
TAPS = 31
EXPERT_UNITS = 2048
CHOSEN = 2
ROUTE_DEV = 128
EXPERTS = 32
CAPACITY = 10
MIX_TOKENS = 16384
ROUTE_TOKENS = 16384
N_EP = 32
N_TP = 4


def draw_mixer_taps(key, part):
    first_key, second_key = jax.random.split(key)
    position = jnp.arange(CHANNELS).astype(jnp.float32) / CHANNELS
    rough = jax.random.uniform(second_key, (CHANNELS,), jnp.float32, 0.5, 2.0)
    factor = jnp.exp(jnp.log(10.0) * position) * rough
    base = jnp.clip(jax.random.normal(first_key, (TAPS, CHANNELS), jnp.float32), -5.0, 5.0) + 0.3
    return (base * factor / math.sqrt(TAPS)).astype(jnp.bfloat16)


def block_levels(own_key, shape, cuts, low, largest):
    level, own = 1.0, jax.random.fold_in(own_key, 6)
    for dim, blocks in cuts:
        draws = jnp.exp(jax.random.uniform(jax.random.fold_in(own, dim), (blocks,), jnp.float32, low / len(cuts), largest / len(cuts)))
        level = level * jnp.repeat(draws, shape[dim] // blocks).reshape([-1 if axis == dim else 1 for axis in range(len(shape))])
    return level


def assign_block(own_key, own, number, rows, number_of, top, bound, skew):
    ranking = jax.random.permutation(own_key, number_of)
    crowded, common = load_shares(number_of, rows * top, bound, skew, True), load_shares(number_of, rows * top, bound, skew, False)
    places = jnp.arange(number_of)

    def named(sizes, turn):
        used = int((sizes > 0).sum())
        fixed = max(1, used // 4)
        moved = fixed + (places - fixed + turn * (used - fixed)) % max(1, number_of - fixed)
        return jnp.zeros((number_of,), jnp.int32).at[ranking[jnp.where(places < fixed, places, moved)]].set(jnp.asarray(sizes, jnp.int32))

    sizes = jnp.where(number % 4 == 0, named(crowded, number // 4), named(common, number - number // 4 - 1))
    mixed = jax.random.permutation(jax.random.fold_in(own, 3), number_of)
    donor, taker = mixed[0:number_of // 2 * 2:2], mixed[1:number_of // 2 * 2:2]
    slack = jnp.minimum(sizes[donor] - 1, bound - sizes[taker]) // 2
    slack = jnp.where((donor == ranking[0]) | (taker == ranking[0]) | (sizes[taker] == 0), 0, jnp.maximum(slack, 0))
    moved = jax.random.randint(jax.random.fold_in(own, 4), (number_of // 2,), 0, 1 << 20) % (slack + 1)
    sizes = sizes.at[donor].add(-moved).at[taker].add(moved)
    labels = jnp.searchsorted(jnp.cumsum(sizes), jnp.arange(rows * top), side="right").astype(jnp.int32)
    grid = labels.reshape(top, rows).T
    grid = grid[jax.random.permutation(jax.random.fold_in(own, 1), rows)]
    turn = jax.random.randint(jax.random.fold_in(own, 2), (rows, 1), 0, top)
    return jnp.take_along_axis(grid, (jnp.arange(top)[None, :] + turn) % top, axis=1)


def load_shares(amount, total, most, slope, full):
    loads = [(1 << 20) // math.isqrt(standing ** slope) + 1 for standing in range(1, amount + 1)]
    largest = most if full else min(most, max(-(-total // amount), total * loads[0] // sum(loads)))
    least = 1 if total - largest >= amount - 1 else 0
    counts, spare = [largest] + [least] * (amount - 1), total - largest - least * (amount - 1)
    while spare > 0:
        free = [i for i in range(1, amount) if counts[i] < largest] or [i for i in range(1, amount) if counts[i] < most]
        pool, left = sum([loads[i] for i in free]), spare
        for i in free:
            more = min(most - counts[i], max(1, left * loads[i] // pool), spare)
            counts[i] = counts[i] + more
            spare = spare - more
    return np.array(counts)


def gaussian(rng, dims, deviation, most, cuts=(), kind=jnp.bfloat16):
    entries = deviation * jax.random.normal(rng, dims, jnp.float32)
    if cuts:
        entries = entries * block_levels(rng, dims, cuts, -0.22, 0.18)
    return jnp.clip(entries, -most, most).astype(kind)


def setup_inputs(seed: int = 0) -> dict:
    key_list = jax.random.split(jax.random.key(seed), 13)
    mixer_value = jnp.clip(-1.0 + 3.0 * jax.random.uniform(key_list[0], (MIX_TOKENS, CHANNELS), jnp.float32) ** block_levels(key_list[0], (MIX_TOKENS, CHANNELS), ((0, 32), (1, 4)), -0.2, 0.2), -1.0, 2.0).astype(jnp.bfloat16)
    mixer_gate = gaussian(key_list[1], (MIX_TOKENS, CHANNELS), 1.0, 6.0, ((0, 32), (1, 4)))
    mixer_taps = draw_mixer_taps(jax.random.fold_in(key_list[12], 71), 0)
    mixer_gain = jnp.clip(1.0 + 0.18 * jax.random.normal(key_list[3], (CHANNELS,), jnp.float32), 0.099609375, 1.8984375).astype(jnp.bfloat16)
    mixer_weight = gaussian(key_list[4], (CHANNELS, WIDTH), CHANNELS ** -0.5, 0.125, ((0, 4),))
    routed_input = gaussian(key_list[5], (ROUTE_TOKENS, WIDTH), 1.0, 6.0, ((0, 32),))
    routed_gain = jnp.clip(1.0 + 0.18 * jax.random.normal(key_list[6], (WIDTH,), jnp.float32), 0.099609375, 1.8984375).astype(jnp.bfloat16)
    expert_ids_keys = jax.random.split(jax.random.fold_in(key_list[7], 1), ROUTE_TOKENS // ROUTE_DEV)
    expert_ids_turns = jax.random.permutation(jax.random.fold_in(key_list[7], 3), ROUTE_TOKENS // ROUTE_DEV)
    expert_ids = jax.vmap(lambda own, number: assign_block(jax.random.fold_in(key_list[7], 2), own, number, ROUTE_DEV, EXPERTS, CHOSEN, CAPACITY, 2))(expert_ids_keys, expert_ids_turns).reshape((ROUTE_TOKENS, CHOSEN))
    route_share = jnp.clip(0.2 + 0.8 * jax.random.uniform(key_list[8], (ROUTE_TOKENS, CHOSEN), jnp.float32) ** block_levels(key_list[8], (ROUTE_TOKENS, CHOSEN), ((0, 32),), -0.2, 0.2), 0.2, 1.0)
    gate_weight = gaussian(key_list[9], (EXPERTS, WIDTH, EXPERT_UNITS), WIDTH ** -0.5, 0.09375, ((0, 32), (2, 4)))
    up_weight = gaussian(key_list[10], (EXPERTS, WIDTH, EXPERT_UNITS), WIDTH ** -0.5, 0.09375, ((0, 32), (2, 4)))
    down_weight = gaussian(key_list[11], (EXPERTS, EXPERT_UNITS, WIDTH), EXPERT_UNITS ** -0.5, 0.125, ((0, 32), (1, 4)))
    return dict(mixer_value=mixer_value, mixer_gate=mixer_gate, mixer_taps=mixer_taps, mixer_gain=mixer_gain, mixer_weight=mixer_weight, routed_input=routed_input, routed_gain=routed_gain, expert_ids=expert_ids, route_share=route_share, gate_weight=gate_weight, up_weight=up_weight, down_weight=down_weight)


def norm_rows(values, gain):
    floats = values.astype(jnp.float32)
    factor = lax.rsqrt(lax.optimization_barrier(jnp.mean(floats * floats, axis=-1, keepdims=True)) + 1e-06)
    return (floats * factor * gain.astype(jnp.float32)).astype(jnp.bfloat16)

def slot_numbers(flat_ids):
    onehot = (flat_ids[..., None] == jnp.arange(EXPERTS, dtype=jnp.int32)).astype(jnp.int32)
    before = jnp.cumsum(onehot, axis=1) - 1
    slot_rank = lax.optimization_barrier(jnp.sum(onehot * before, axis=-1))
    return flat_ids * CAPACITY + slot_rank

def reference(mixer_value, mixer_gate, mixer_taps, mixer_gain, mixer_weight, routed_input, routed_gain, expert_ids, route_share, gate_weight, up_weight, down_weight):
    gated = (mixer_value.astype(jnp.float32) * jax.nn.sigmoid(mixer_gate.astype(jnp.float32))).astype(jnp.bfloat16)
    length = gated.shape[0]
    extended = jnp.concatenate([jnp.zeros((TAPS - 1, CHANNELS), jnp.float32), gated.astype(jnp.float32)], axis=0)
    taps_float = mixer_taps.astype(jnp.float32)
    filtered = taps_float[0] * extended[0:length]
    for offset in range(1, TAPS):
        filtered = filtered + taps_float[offset] * extended[offset:offset + length]
    center = lax.optimization_barrier(jnp.sum(filtered, axis=1)) / CHANNELS
    spread = lax.optimization_barrier(jnp.sum(filtered * filtered, axis=1)) / CHANNELS - center * center
    normed_mix = (filtered - center[:, None]) * lax.rsqrt(spread + 1e-05)[:, None] * mixer_gain.astype(jnp.float32)
    mixer_hidden = jax.nn.silu(normed_mix).astype(jnp.bfloat16)
    group = CHANNELS // N_TP
    mixer_sum = jnp.zeros((length, WIDTH), jnp.float32)
    for quarter in range(N_TP):
        partial_part = jnp.dot(mixer_hidden[:, quarter * group:(quarter + 1) * group], mixer_weight[quarter * group:(quarter + 1) * group], preferred_element_type=jnp.float32).astype(jnp.bfloat16)
        partial_part = lax.optimization_barrier(partial_part)
        mixer_sum = mixer_sum + partial_part.astype(jnp.float32)
    mixer_result = mixer_sum.astype(jnp.bfloat16)
    blocks = N_EP * N_TP
    normed = norm_rows(routed_input, routed_gain).reshape(blocks, ROUTE_DEV, WIDTH)
    flat_ids = expert_ids.reshape(blocks, ROUTE_DEV * CHOSEN)
    slot_ids = slot_numbers(flat_ids)
    owners = jnp.arange(ROUTE_DEV * CHOSEN, dtype=jnp.int32) // CHOSEN
    source_rows = normed[:, owners]
    block_ids = jnp.arange(blocks, dtype=jnp.int32)[:, None]
    buffer = jnp.zeros((blocks, EXPERTS * CAPACITY, WIDTH), jnp.bfloat16).at[block_ids, slot_ids].set(source_rows)
    per_expert = buffer.reshape(blocks, EXPERTS, CAPACITY, WIDTH).transpose(1, 0, 2, 3).reshape(EXPERTS, blocks * CAPACITY, WIDTH)
    hidden_group = EXPERT_UNITS // N_TP

    def one_expert(packed):
        rows_in, gate_mat, up_mat, down_mat = packed
        gate_part = jnp.dot(rows_in, gate_mat, preferred_element_type=jnp.float32)
        up_part = jnp.dot(rows_in, up_mat, preferred_element_type=jnp.float32)
        hidden_rows = (jax.nn.silu(gate_part) * up_part).astype(jnp.bfloat16)
        total = jnp.zeros((rows_in.shape[0], WIDTH), jnp.float32)
        for quarter in range(N_TP):
            piece = jnp.dot(hidden_rows[:, quarter * hidden_group:(quarter + 1) * hidden_group], down_mat[quarter * hidden_group:(quarter + 1) * hidden_group], preferred_element_type=jnp.float32).astype(jnp.bfloat16)
            piece = lax.optimization_barrier(piece)
            total = total + piece.astype(jnp.float32)
        return total.astype(jnp.bfloat16)
    outputs = lax.map(one_expert, (per_expert, gate_weight, up_weight, down_weight))
    returned = outputs.reshape(EXPERTS, blocks, CAPACITY, WIDTH).transpose(1, 0, 2, 3).reshape(blocks, EXPERTS * CAPACITY, WIDTH)
    picked = jnp.take_along_axis(returned, slot_ids[..., None], axis=1).astype(jnp.float32).reshape(blocks, ROUTE_DEV, CHOSEN, WIDTH)
    shares = route_share.reshape(blocks, ROUTE_DEV, CHOSEN)
    routed_result = lax.optimization_barrier(jnp.sum(shares[..., None] * picked, axis=2)).reshape(ROUTE_TOKENS, WIDTH).astype(jnp.bfloat16)
    return (mixer_result, routed_result)
```

```python
import jax
import jax.numpy as jnp
from jax import lax
from jax.sharding import PartitionSpec as P

RETURN_PIECES = 2
f32 = jnp.float32
bf16 = jnp.bfloat16


def turned(value, axis, steps):
    count = lax.axis_size(axis)
    return lax.ppermute(value, axis, [(i, (i + steps) % count) for i in range(count)])


def dot(a, b):
    return jnp.dot(a, b, preferred_element_type=f32)


def on_device(
    mixer_value,
    mixer_gate,
    mixer_taps,
    mixer_gain,
    mixer_weight,
    routed_input,
    routed_gain,
    expert_ids,
    route_share,
    gate_weight,
    up_weight,
    down_weight,
):
    parts = lax.axis_size("tp")
    sources = lax.axis_size("ep")
    q = lax.axis_index("tp")
    right, across, left = (q + 1) % parts, (q + 2) % parts, (q + 3) % parts
    rows, width = routed_input.shape
    block = rows // parts
    chosen = expert_ids.shape[1]
    capacity = 5 * block // (2 * sources)
    per_source = parts * capacity
    slots = sources * per_source
    quarter = width // parts

    ids = expert_ids.T.reshape(chosen, parts, block)
    earlier = jnp.arange(block)[:, None] < jnp.arange(block)[None, :]
    same = ids[:, None, :, :, None] == ids[None, :, :, None, :]
    rank = jnp.sum((same & earlier).astype(jnp.int32), axis=(0, 3))

    code = ids * per_source + jnp.arange(parts, dtype=jnp.int32)[None, :, None] * capacity + rank
    code = code.reshape(chosen, rows)
    slot_row = jnp.arange(slots, dtype=jnp.int32)[:, None]
    picks = (slot_row == code[0][None]) | (slot_row == code[1][None])
    picks = picks.astype(bf16)

    floats = routed_input.astype(f32)
    factor = lax.rsqrt(jnp.mean(floats * floats, axis=-1, keepdims=True) + 1e-06)

    def dispatched(start, size):
        piece = lax.dynamic_slice_in_dim(routed_input, start, size, 1).astype(f32)
        gain = lax.dynamic_slice_in_dim(routed_gain, start, size, 0).astype(f32)
        normed = (piece * factor * gain).astype(bf16)
        outgoing = dot(picks, normed).astype(bf16).reshape(sources, per_source, size)
        return lax.all_to_all(outgoing, "ep", 0, 0, tiled=True).reshape(slots, size)

    half = quarter // 2
    own = [dispatched(q * quarter + k * half, half) for k in range(2)]
    far = dispatched(across * quarter, quarter)
    held = []
    for k in range(2):
        held.append((own[k], q * quarter + k * half))
        held.append((turned(own[k], "tp", 1), left * quarter + k * half))
        held.append((turned(own[k], "tp", -1), right * quarter + k * half))
    held.append((far, across * quarter))

    taps = mixer_taps.shape[0]
    length = mixer_value.shape[0]
    gated = (mixer_value.astype(f32) * jax.nn.sigmoid(mixer_gate.astype(f32))).astype(bf16)
    before = lax.ppermute(
        gated[length - (taps - 1) :], "ep", [(i, i + 1) for i in range(sources - 1)]
    )
    extended = jnp.concatenate([before, gated], axis=0).astype(f32)
    taps_float = mixer_taps.astype(f32)
    filtered = taps_float[0] * extended[0:length]
    for offset in range(1, taps):
        filtered = filtered + taps_float[offset] * extended[offset : offset + length]
    stats = jnp.stack([jnp.sum(filtered, axis=1), jnp.sum(filtered * filtered, axis=1)])
    stats = (
        stats + turned(stats, "tp", 1) + turned(stats, "tp", -1) + turned(stats, "tp", 2)
    )
    channels = mixer_taps.shape[1] * parts
    center = stats[0] / channels
    spread = stats[1] / channels - center * center
    normed_mix = (
        (filtered - center[:, None])
        * lax.rsqrt(spread + 1e-05)[:, None]
        * mixer_gain.astype(f32)
    )
    mixer_hidden = jax.nn.silu(normed_mix).astype(bf16)
    mix_block = length // parts

    def mixed(index):
        piece = lax.dynamic_slice_in_dim(mixer_hidden, index * mix_block, mix_block, 0)
        return dot(piece, mixer_weight)

    middle = width // 2
    mix_far = mixed(across).astype(bf16)
    via_right = turned(mix_far[:, :middle], "tp", 1).astype(f32)
    via_left = turned(mix_far[:, middle:], "tp", -1).astype(f32)
    mix_right, mix_left = mixed(right), mixed(left)
    to_right = jnp.concatenate([mix_right[:, :middle] + via_right, mix_right[:, middle:]], axis=1)
    to_left = jnp.concatenate([mix_left[:, :middle], mix_left[:, middle:] + via_left], axis=1)
    from_left = turned(to_right.astype(bf16), "tp", 1).astype(f32)
    from_right = turned(to_left.astype(bf16), "tp", -1).astype(f32)
    mixer_result = (mixed(q) + from_left + from_right).astype(bf16)

    def projected(weight):
        total = None
        for piece, start in held:
            part = dot(piece, lax.dynamic_slice_in_dim(weight, start, piece.shape[1], 0))
            total = part if total is None else total + part
        return total

    gate_part = projected(gate_weight[0])
    up_part = projected(up_weight[0])
    hidden = (jax.nn.silu(gate_part) * up_part).astype(bf16)

    block_slots = sources * capacity
    row = jnp.arange(block_slots, dtype=jnp.int32)[:, None]
    place = (row // capacity) * per_source + row % capacity
    column = jnp.arange(slots, dtype=jnp.int32)[None, :]

    def hidden_of(index):
        return dot((column == place + index * capacity).astype(bf16), hidden).astype(bf16)

    piece_width = width // RETURN_PIECES
    fold = piece_width // parts

    def messages(value):
        value = value.reshape(sources, capacity, parts, fold).transpose(0, 2, 1, 3)
        return value.reshape(sources, per_source, fold)

    def shares_of(index):
        own_ids = lax.dynamic_slice_in_dim(ids, index, 1, 1)[:, 0]
        own_rank = lax.dynamic_slice_in_dim(rank, index, 1, 1)[:, 0]
        own_share = lax.dynamic_slice_in_dim(route_share, index * block, block, 0).T
        home = (own_ids * per_source + own_rank)[:, None, :]
        home = home + jnp.arange(parts, dtype=jnp.int32)[None, :, None] * capacity
        home = home.reshape(chosen, parts * block, 1)
        weight = jnp.broadcast_to(own_share[:, None, :], (chosen, parts, block))
        weight = weight.reshape(chosen, parts * block, 1)
        total = jnp.where(column == home[0], weight[0], 0.0)
        total = total + jnp.where(column == home[1], weight[1], 0.0)
        return total.astype(bf16)

    def combined(received, shares):
        total = dot(shares, received.reshape(slots, fold)).reshape(parts, block, fold)
        return total.transpose(1, 0, 2).reshape(block, parts * fold)

    def back(value):
        return lax.all_to_all(messages(value), "ep", 0, 0, tiled=True)

    hid = {name: hidden_of(index) for name, index in
           (("right", right), ("left", left), ("far", across), ("own", q))}
    shares_far, shares_own = shares_of(across), shares_of(q)
    outs = []
    for k in range(RETURN_PIECES):
        down = down_weight[0][:, k * piece_width : (k + 1) * piece_width]
        from_left = turned(dot(hid["right"], down).astype(bf16), "tp", 1)
        from_right = turned(dot(hid["left"], down).astype(bf16), "tp", -1)
        far_back = back(dot(hid["far"], down).astype(bf16))
        far_rows = combined(far_back, shares_far).astype(bf16)
        far_rows = turned(far_rows, "tp", 2)
        own_rows = dot(hid["own"], down) + from_left.astype(f32) + from_right.astype(f32)
        own_back = back(own_rows.astype(bf16))
        outs.append((combined(own_back, shares_own) + far_rows.astype(f32)).astype(bf16))
    return (mixer_result, jnp.concatenate(outs, axis=1))


def solution(mesh):
    return jax.shard_map(
        on_device,
        mesh=mesh,
        in_specs=(
            P("ep", "tp"),
            P("ep", "tp"),
            P(None, "tp"),
            P("tp"),
            P("tp", None),
            P("ep", None),
            P(),
            P("ep", None),
            P("ep", None),
            P("ep", None, "tp"),
            P("ep", None, "tp"),
            P("ep", "tp", None),
        ),
        out_specs=(P(("ep", "tp"), None), P(("ep", "tp"), None)),
        check_vma=False,
    )
```

```python
import functools

import jax
import jax.numpy as jnp
from jax import lax
from jax.experimental import pallas as pl
from jax.experimental.pallas import tpu as pltpu
from jax.sharding import PartitionSpec as P


RETURN_PIECES = 2
f32 = jnp.float32
bf16 = jnp.bfloat16
i32 = jnp.int32


def turned(value, axis, steps):
    count = lax.axis_size(axis)
    return lax.ppermute(value, axis, [(i, (i + steps) % count) for i in range(count)])


def dot(a, b):
    return jnp.dot(a, b, preferred_element_type=f32)


def call(body, grid, ins, outs, scratch=(), flops=0, moved=0, prefetch=1):
    return pl.pallas_call(
        body,
        out_shape=[jax.ShapeDtypeStruct(shape, kind) for shape, kind, _ in outs],
        grid_spec=pltpu.PrefetchScalarGridSpec(
            num_scalar_prefetch=prefetch,
            grid=grid,
            in_specs=ins,
            out_specs=[spec for _, _, spec in outs],
            scratch_shapes=list(scratch),
        ),
        cost_estimate=pl.CostEstimate(flops=flops, bytes_accessed=moved, transcendentals=0),
    )


def whole(shape):
    return pl.BlockSpec(shape, lambda *_: (0,) * len(shape), pipeline_mode=pl.Buffered(1))


def one_hot_rows(code_ref, slots, rows, tile=0):
    slot = lax.broadcasted_iota(i32, (slots, rows), 0) + tile * slots
    picks = (slot == code_ref[0:1, :]) | (slot == code_ref[1:2, :])
    return jnp.where(picks, 1.0, 0.0).astype(bf16)


def near_body(q_ref, code_ref, x_ref, gain_ref, out_ref, factor_ref, normed_ref, *, quarter, half):
    step = pl.program_id(0)
    block, width = x_ref.shape
    side = out_ref.shape[1]

    @pl.when(step < half)
    def _():
        x = x_ref[...].astype(f32)
        factor = lax.rsqrt(jnp.sum(x * x, axis=1, keepdims=True) / width + 1e-06)
        factor_ref[...] = jnp.broadcast_to(factor, factor_ref.shape)
        columns = pl.ds(pl.multiple_of(q_ref[0] * quarter, quarter), side)
        piece = x_ref[:, columns].astype(f32) * factor * gain_ref[:, columns].astype(f32)
        normed_ref[pl.ds(step * block, block), :] = piece.astype(bf16)

    @pl.when(step >= half)
    def _():
        picks = one_hot_rows(code_ref, out_ref.shape[0], normed_ref.shape[0], step - half)
        out_ref[...] = dot(picks, normed_ref[...]).astype(bf16)


def near_rows(index, code, x, gain, slots, side):
    rows, width = x.shape
    quarter = width // 4
    half = 4
    block, tile = rows // half, slots // half
    return call(
        functools.partial(near_body, quarter=quarter, half=half),
        (2 * half,),
        [
            whole(code.shape),
            pl.BlockSpec((block, width), lambda i, q: (jnp.minimum(i, half - 1), 0)),
            whole(gain.shape),
        ],
        [
            (
                (slots, side),
                bf16,
                pl.BlockSpec((tile, side), lambda i, q: (jnp.maximum(i - half, 0), 0)),
            ),
            (
                (rows, 128),
                f32,
                pl.BlockSpec((block, 128), lambda i, q: (jnp.minimum(i, half - 1), 0)),
            ),
        ],
        [pltpu.VMEM((rows, side), bf16)],
        2 * slots * rows * side,
        2 * (rows * width + slots * side),
    )(index, code, x, gain)


def far_body(q_ref, code_ref, x0, x1, x2, x3, g0, g1, g2, g3, factor_ref, out_ref, normed_ref):
    @pl.when(pl.program_id(0) == 0)
    def _():
        at = 0
        for x_ref, gain_ref in ((x0, g0), (x1, g1), (x2, g2), (x3, g3)):
            size = x_ref.shape[1]
            piece = x_ref[...].astype(f32) * factor_ref[:, 0:1] * gain_ref[...].astype(f32)
            normed_ref[:, at : at + size] = piece.astype(bf16)
            at += size

    picks = one_hot_rows(code_ref, out_ref.shape[0], normed_ref.shape[0], pl.program_id(0))
    out_ref[...] = dot(picks, normed_ref[...]).astype(bf16)


def far_rows(index, code, x, gain, factor, slots, side):
    rows, width = x.shape
    quarter = width // 4
    rest = quarter - side
    each = quarter // rest
    total = quarter + 3 * rest
    steps = 4

    def last(step):
        return (rest, lambda i, q: (0, (q[0] + step) % 4 * each + each - 1))

    places = [(quarter, lambda i, q: (0, (q[0] + 2) % 4)), last(0), last(1), last(3)]
    once = pl.Buffered(1)
    return call(
        far_body,
        (steps,),
        [whole(code.shape)]
        + [pl.BlockSpec((rows, size), place, pipeline_mode=once) for size, place in places]
        + [pl.BlockSpec((1, size), place, pipeline_mode=once) for size, place in places]
        + [whole(factor.shape)],
        [((slots, total), bf16, pl.BlockSpec((slots // steps, total), lambda i, q: (i, 0)))],
        [pltpu.VMEM((rows, total), bf16)],
        2 * slots * rows * total,
        2 * (rows + slots) * total,
    )(index, code, x, x, x, x, gain, gain, gain, gain, factor)[0]


def first_body(q_ref, x_ref, wg_ref, wu_ref, gate_ref, up_ref):
    gate_ref[...] = dot(x_ref[...], wg_ref[...])
    up_ref[...] = dot(x_ref[...], wu_ref[...])


def first_part(index, x, wg, wu):
    slots, side = x.shape
    units = wg.shape[1]
    quarter = wg.shape[0] // 4
    tile = slots // 4
    weight = pl.BlockSpec(
        (pl.Element(side), pl.Element(units)),
        lambda i, q: (q[0] * quarter, 0),
        pipeline_mode=pl.Buffered(1),
    )
    rowed = pl.BlockSpec((tile, units), lambda i, q: (i, 0))
    return call(
        first_body,
        (4,),
        [pl.BlockSpec((tile, side), lambda i, q: (i, 0)), weight, weight],
        [((slots, units), f32, rowed), ((slots, units), f32, rowed)],
        (),
        4 * slots * side * units,
        2 * slots * side + 4 * side * units + 8 * slots * units,
    )(index, x, wg, wu)


def hidden_body(q_ref, far_ref, right_ref, left_ref, gate_ref, up_ref, *refs, capacity):
    weights, out_ref = refs[:-1], refs[-1]
    many = len(weights) // 2
    parts, count, units = out_ref.shape
    size = parts * count

    def total(start_ref, own):
        value = start_ref[...] + dot(right_ref[...], own[0][...]) + dot(left_ref[...], own[1][...])
        at = 0
        for weight_ref in own[2:]:
            rows = weight_ref.shape[0]
            value += dot(far_ref[:, at : at + rows], weight_ref[...])
            at += rows
        return value

    gate = total(gate_ref, weights[:many])
    up = total(up_ref, weights[many:])
    hidden = (gate / (1.0 + jnp.exp(-gate)) * up).astype(bf16)
    row = lax.broadcasted_iota(i32, (size, 1), 0)
    place = row % count // capacity * (parts * capacity) + row // count * capacity + row % capacity
    column = lax.broadcasted_iota(i32, (size, size), 1)
    order = jnp.where(column == place, 1.0, 0.0).astype(bf16)
    out_ref[...] = dot(order, hidden).astype(bf16).reshape(parts, count, units)


def hidden_units(index, far, right, left, gate, up, wg, wu, capacity):
    slots, side = right.shape
    units = wg.shape[1]
    quarter = wg.shape[0] // 4
    rest = quarter - side
    each = quarter // rest
    steps, parts = 4, 4
    tile = slots // steps
    once = pl.Buffered(1)

    def lent(step):
        return pl.BlockSpec(
            (pl.Element(side), pl.Element(units)),
            lambda i, q: ((q[0] + step) % 4 * quarter, 0),
            pipeline_mode=once,
        )

    def last(step):
        return pl.BlockSpec(
            (rest, units),
            lambda i, q: ((q[0] + step) % 4 * each + each - 1, 0),
            pipeline_mode=once,
        )

    weights = [
        lent(1),
        lent(3),
        pl.BlockSpec((quarter, units), lambda i, q: ((q[0] + 2) % 4, 0), pipeline_mode=once),
        last(0),
        last(1),
        last(3),
    ]
    depth = far.shape[1] + 2 * side

    def rowed(size):
        return pl.BlockSpec((tile, size), lambda i, q: (i, 0))

    return call(
        functools.partial(hidden_body, capacity=capacity),
        (steps,),
        [rowed(far.shape[1]), rowed(side), rowed(side), rowed(units), rowed(units)] + weights * 2,
        [
            (
                (parts, slots // parts, units),
                bf16,
                pl.BlockSpec((parts, tile // parts, units), lambda i, q: (0, i, 0)),
            )
        ],
        (),
        4 * slots * depth * units,
        2 * slots * depth + 4 * depth * units + 10 * slots * units,
    )(index, far, right, left, gate, up, *[wg] * 6, *[wu] * 6)[0]


def rows_of(hidden, step):
    parts, count, units = hidden.shape
    return pl.BlockSpec(
        (None, count, units), lambda i, q: ((q[0] + step) % parts, 0, 0), pipeline_mode=pl.Buffered(1)
    )


def sides_body(q_ref, to_right_ref, to_left_ref, down_ref, right_ref, left_ref):
    right_ref[...] = dot(to_right_ref[...], down_ref[...]).astype(bf16)
    left_ref[...] = dot(to_left_ref[...], down_ref[...]).astype(bf16)


def side_rows(index, hidden, down, piece, pieces):
    _, count, units = hidden.shape
    width = down.shape[1] // pieces
    steps = 4
    tile = width // steps
    tiled = pl.BlockSpec((count, tile), lambda i, q: (0, i))
    return call(
        sides_body,
        (steps,),
        [
            rows_of(hidden, 1),
            rows_of(hidden, 3),
            pl.BlockSpec((units, tile), lambda i, q: (0, piece * steps + i)),
        ],
        [((count, width), bf16, tiled), ((count, width), bf16, tiled)],
        (),
        4 * count * units * width,
        2 * (2 * count * units + units * width + 2 * count * width),
    )(index, hidden, hidden, down)


def own_body(q_ref, rows_ref, down_ref, out_ref):
    out_ref[...] = dot(rows_ref[...], down_ref[...]).astype(bf16)


def own_rows(index, hidden, down, piece, pieces):
    _, count, units = hidden.shape
    width = down.shape[1] // pieces
    steps = 4
    tile = width // steps
    return call(
        own_body,
        (steps,),
        [
            rows_of(hidden, 0),
            pl.BlockSpec((units, tile), lambda i, q: (0, piece * steps + i)),
        ],
        [((count, width), bf16, pl.BlockSpec((count, tile), lambda i, q: (0, i)))],
        (),
        2 * count * units * width,
        2 * (count * units + units * width + count * width),
    )(index, hidden, down)[0]


def messages_of(value, fold, capacity, parts):
    many = value.shape[0]
    size, each = many * parts, parts * capacity
    row = lax.broadcasted_iota(i32, (size, 1), 0)
    place = row % each // capacity * many + row // each * capacity + row % capacity
    column = lax.broadcasted_iota(i32, (size, size), 1)
    order = jnp.where(column == place, 1.0, 0.0).astype(bf16)
    stack = jnp.concatenate([value[:, k * fold : (k + 1) * fold] for k in range(parts)], axis=0)
    return dot(order, stack).astype(bf16)


def across_body(q_ref, rows_ref, down_ref, out_ref, value_ref, *, capacity, parts, steps):
    step = pl.program_id(0)
    tile, fold, many = down_ref.shape[1], out_ref.shape[1], out_ref.shape[0] // parts

    @pl.when(step < steps)
    def _():
        columns = pl.ds(pl.multiple_of(step * tile, tile), tile)
        value_ref[:, columns] = dot(rows_ref[...], down_ref[...]).astype(bf16)

    @pl.when(step >= steps)
    def _():
        value = value_ref[pl.ds(pl.multiple_of((step - steps) * many, many), many), :]
        out_ref[...] = messages_of(value, fold, capacity, parts)


def across_messages(index, hidden, down, piece, pieces, capacity):
    parts, count, units = hidden.shape
    width = down.shape[1] // pieces
    slots, fold = parts * count, width // parts
    steps = 4
    tile = width // steps
    return call(
        functools.partial(across_body, capacity=capacity, parts=parts, steps=steps),
        (2 * steps,),
        [
            rows_of(hidden, 2),
            pl.BlockSpec(
                (units, tile), lambda i, q: (0, piece * steps + jnp.minimum(i, steps - 1))
            ),
        ],
        [
            (
                (slots, fold),
                bf16,
                pl.BlockSpec((slots // steps, fold), lambda i, q: (jnp.maximum(i - steps, 0), 0)),
            )
        ],
        [pltpu.VMEM((count, width), bf16)],
        2 * count * units * width,
        2 * (count * units + units * width + count * width),
    )(index, hidden, down)[0]


def summed_body(q_ref, own_ref, left_ref, right_ref, out_ref, *, capacity, parts):
    total = own_ref[...].astype(f32) + left_ref[...].astype(f32) + right_ref[...].astype(f32)
    out_ref[...] = messages_of(total.astype(bf16), out_ref.shape[1], capacity, parts)


def summed_messages(index, own, left, right, capacity, parts):
    count, width = own.shape
    slots, fold = count * parts, width // parts
    steps = 4
    rowed = pl.BlockSpec((count // steps, width), lambda i, q: (i, 0))
    return call(
        functools.partial(summed_body, capacity=capacity, parts=parts),
        (steps,),
        [rowed, rowed, rowed],
        [((slots, fold), bf16, pl.BlockSpec((slots // steps, fold), lambda i, q: (i, 0)))],
        (),
        2 * slots * slots // 4 * fold,
        8 * count * width,
    )(index, own, left, right)[0]


def combine_body(q_ref, home_ref, share_ref, rows_ref, *refs, capacity, parts):
    out_ref, weight_ref, value_ref = refs[-3:]
    extra = refs[0] if len(refs) > 3 else None
    step = pl.program_id(0)
    slots, tile = rows_ref.shape
    block, width = out_ref.shape

    @pl.when(step == 0)
    def _():
        column = lax.broadcasted_iota(i32, (block, slots), 1)
        for k in range(parts):
            home = home_ref[...] + k * capacity
            weights = jnp.where(column == home[:, 0:1], share_ref[:, 0:1], 0.0)
            weights = jnp.where(column == home[:, 1:2], share_ref[:, 1:2], weights)
            weight_ref[k * block : (k + 1) * block, :] = weights.astype(bf16)

    value_ref[...] = dot(weight_ref[...], rows_ref[...])
    for k in range(parts):
        columns = pl.ds(pl.multiple_of(k * (width // parts) + step * tile, tile), tile)
        value = value_ref[k * block : (k + 1) * block, :]
        if extra is not None:
            value = value + extra[:, columns].astype(f32)
        out_ref[:, columns] = value.astype(bf16)


def combined(index, home, share, rows, capacity, parts, extra=None, into=None, piece=0, pieces=1):
    slots, fold = rows.shape
    block = home.shape[0]
    width = parts * fold
    steps = 2
    placed = pl.BlockSpec((block, width), lambda i, q: (0, piece), pipeline_mode=pl.Buffered(1))
    ins = [
        whole(home.shape),
        whole(share.shape),
        pl.BlockSpec((slots, fold // steps), lambda i, q: (0, i)),
    ]
    args = [home, share, rows]
    if extra is not None:
        ins.append(placed)
        args.append(extra)
    if into is not None:
        ins.append(pl.BlockSpec(memory_space=pl.ANY))
        args.append(into)
    return pl.pallas_call(
        functools.partial(combine_body, capacity=capacity, parts=parts),
        out_shape=jax.ShapeDtypeStruct((block, width * pieces), bf16),
        grid_spec=pltpu.PrefetchScalarGridSpec(
            num_scalar_prefetch=1,
            grid=(steps,),
            in_specs=ins,
            out_specs=placed,
            scratch_shapes=[
                pltpu.VMEM((parts * block, slots), bf16),
                pltpu.VMEM((parts * block, fold // steps), f32),
            ],
        ),
        input_output_aliases={} if into is None else {len(args): 0},
        cost_estimate=pl.CostEstimate(
            flops=2 * parts * block * slots * fold,
            bytes_accessed=2 * slots * fold + 4 * block * width,
            transcendentals=0,
        ),
        name="combined",
    )(index, *args)


def mixed_body(q_ref, hidden_ref, weight_ref, own_ref, *outs):
    step = pl.program_id(0)
    parts = 4
    block = own_ref.shape[0]
    middle = pl.num_programs(0) // 2

    def rows_for(which):
        start = pl.multiple_of((q_ref[0] + which) % parts * block, block)
        return dot(hidden_ref[pl.ds(start, block), :], weight_ref[...]).astype(bf16)

    own_ref[...] = rows_for(0)

    @pl.when(step < middle)
    def _():
        for k in range(parts - 1):
            outs[2 * k][...] = rows_for(k + 1)

    @pl.when(step >= middle)
    def _():
        for k in range(parts - 1):
            outs[2 * k + 1][...] = rows_for(k + 1)


def mixed_rows(index, hidden, weight, parts):
    rows, channels = hidden.shape
    width = weight.shape[1]
    steps = 4
    block, tile = rows // parts, width // steps
    low = pl.BlockSpec((block, tile), lambda i, q: (0, jnp.minimum(i, steps // 2 - 1)))
    high = pl.BlockSpec((block, tile), lambda i, q: (0, jnp.maximum(i - steps // 2, 0)))
    return call(
        mixed_body,
        (steps,),
        [whole(hidden.shape), pl.BlockSpec((channels, tile), lambda i, q: (0, i))],
        [((block, width), bf16, pl.BlockSpec((block, tile), lambda i, q: (0, i)))]
        + [((block, width // 2), bf16, low), ((block, width // 2), bf16, high)] * (parts - 1),
        (),
        2 * rows * channels * width,
        2 * (rows * channels + channels * width + rows * width),
    )(index, hidden, weight)


def on_device(
    mixer_value,
    mixer_gate,
    mixer_taps,
    mixer_gain,
    mixer_weight,
    routed_input,
    routed_gain,
    expert_ids,
    route_share,
    gate_weight,
    up_weight,
    down_weight,
):
    parts = lax.axis_size("tp")
    sources = lax.axis_size("ep")
    q = lax.axis_index("tp").astype(i32)
    index = q.reshape(1)
    across = (q + 2) % parts
    rows, width = routed_input.shape
    block = rows // parts
    chosen = expert_ids.shape[1]
    capacity = 5 * block // (2 * sources)
    per_source = parts * capacity
    slots = sources * per_source
    quarter = width // parts
    side = 7 * quarter // 8

    ids = expert_ids.T.reshape(chosen, parts, block)
    earlier = jnp.arange(block)[:, None] < jnp.arange(block)[None, :]
    same = ids[:, None, :, :, None] == ids[None, :, :, None, :]
    rank = jnp.sum((same & earlier).astype(i32), axis=(0, 3))
    code = ids * per_source + jnp.arange(parts, dtype=i32)[None, :, None] * capacity + rank
    code = code.reshape(chosen, rows)

    def exchanged(messages):
        size = messages.shape[1]
        messages = messages.reshape(sources, per_source, size)
        return lax.all_to_all(messages, "ep", 0, 0, tiled=True).reshape(slots, size)

    taps = mixer_taps.shape[0]
    length = mixer_value.shape[0]
    gated = (mixer_value.astype(f32) * jax.nn.sigmoid(mixer_gate.astype(f32))).astype(bf16)
    before = lax.ppermute(
        gated[length - (taps - 1) :], "ep", [(i, i + 1) for i in range(sources - 1)]
    )

    gain = routed_gain.reshape(1, width)
    near, factor = near_rows(index, code, routed_input, gain, slots, side)
    near, before = lax.optimization_barrier((near, before))
    near = exchanged(near)

    extended = jnp.concatenate([before, gated], axis=0).astype(f32)
    taps_float = mixer_taps.astype(f32)
    filtered = taps_float[0] * extended[0:length]
    for offset in range(1, taps):
        filtered = filtered + taps_float[offset] * extended[offset : offset + length]
    stats = jnp.stack([jnp.sum(filtered, axis=1), jnp.sum(filtered * filtered, axis=1)])
    stats = stats + turned(stats, "tp", 1) + turned(stats, "tp", -1) + turned(stats, "tp", 2)
    channels = mixer_taps.shape[1] * parts
    center = stats[0] / channels
    spread = stats[1] / channels - center * center
    normed_mix = (
        (filtered - center[:, None])
        * lax.rsqrt(spread + 1e-05)[:, None]
        * mixer_gain.astype(f32)
    )
    mixer_hidden = jax.nn.silu(normed_mix).astype(bf16)
    mix_own, right_low, right_high, far_low, far_high, left_low, left_high = mixed_rows(
        index, mixer_hidden, mixer_weight, parts
    )
    via_right, via_left = turned(far_low, "tp", 1), turned(far_high, "tp", -1)
    raw_high, raw_low = turned(right_high, "tp", 1), turned(left_low, "tp", -1)

    factor, right_low, left_high = lax.optimization_barrier((factor, right_low, left_high))
    far = far_rows(index, code, routed_input, gain, factor, slots, side)
    from_left, from_right = turned(near, "tp", 1), turned(near, "tp", -1)
    far = exchanged(far)

    gate, up = first_part(index, near, gate_weight[0], up_weight[0])
    hidden = hidden_units(
        index, far, from_right, from_left, gate, up, gate_weight[0], up_weight[0], capacity
    )

    hidden, right_low, left_high = lax.optimization_barrier((hidden, right_low, left_high))
    sum_low = turned((right_low.astype(f32) + via_right.astype(f32)).astype(bf16), "tp", 1)
    sum_high = turned((left_high.astype(f32) + via_left.astype(f32)).astype(bf16), "tp", -1)
    middle = width // 2
    mixer_result = jnp.concatenate(
        [
            mix_own[:, :middle].astype(f32) + sum_low.astype(f32) + raw_low.astype(f32),
            mix_own[:, middle:].astype(f32) + sum_high.astype(f32) + raw_high.astype(f32),
        ],
        axis=1,
    ).astype(bf16)

    def home_of(which):
        own_ids = lax.dynamic_slice_in_dim(ids, which, 1, 1)[:, 0]
        own_rank = lax.dynamic_slice_in_dim(rank, which, 1, 1)[:, 0]
        own_share = lax.dynamic_slice_in_dim(route_share, which * block, block, 0)
        return (own_ids * per_source + own_rank).T, own_share

    down = down_weight[0]
    far_home, own_home = home_of(across), home_of(q)
    pieces = RETURN_PIECES
    got = []
    for piece in range(pieces):
        to_right, to_left = side_rows(index, hidden, down, piece, pieces)
        got.append((turned(to_right, "tp", 1), turned(to_left, "tp", -1)))
    messages = across_messages(index, hidden, down, 0, 1, capacity)
    far_back = exchanged(messages)
    extra = combined(index, *far_home, far_back, capacity, parts)
    own = [own_rows(index, hidden, down, piece, pieces) for piece in range(pieces)]
    extra, own[-1] = lax.optimization_barrier((extra, own[-1]))
    extra = turned(extra, "tp", 2)
    result = None
    for piece in range(pieces):
        messages = summed_messages(index, own[piece], *got[piece], capacity, parts)
        back = exchanged(messages)
        result = combined(
            index, *own_home, back, capacity, parts, extra, result, piece, pieces
        )
    return (mixer_result, result)


def solution(mesh):
    return jax.shard_map(
        on_device,
        mesh=mesh,
        in_specs=(
            P("ep", "tp"),
            P("ep", "tp"),
            P(None, "tp"),
            P("tp"),
            P("tp", None),
            P("ep", None),
            P(),
            P("ep", None),
            P("ep", None),
            P("ep", None, "tp"),
            P("ep", None, "tp"),
            P("ep", "tp", None),
        ),
        out_specs=(P(("ep", "tp"), None), P(("ep", "tp"), None)),
        check_vma=False,
    )
```

```python
import functools

import jax
import jax.numpy as jnp
from jax import lax
from jax.experimental import pallas as pl
from jax.experimental.pallas import tpu as pltpu
from jax.sharding import PartitionSpec as P


PIECES = 2
f32 = jnp.float32
bf16 = jnp.bfloat16
i32 = jnp.int32


def turned(value, axis, steps):
    count = lax.axis_size(axis)
    return lax.ppermute(value, axis, [(i, (i + steps) % count) for i in range(count)])


def dot(a, b):
    return jnp.dot(a, b, preferred_element_type=f32)


def call(body, grid, ins, outs, scratch=(), flops=0, moved=0, prefetch=1):
    return pl.pallas_call(
        body,
        out_shape=[jax.ShapeDtypeStruct(shape, kind) for shape, kind, _ in outs],
        grid_spec=pltpu.PrefetchScalarGridSpec(
            num_scalar_prefetch=prefetch,
            grid=grid,
            in_specs=ins,
            out_specs=[spec for _, _, spec in outs],
            scratch_shapes=list(scratch),
        ),
        cost_estimate=pl.CostEstimate(flops=flops, bytes_accessed=moved, transcendentals=0),
    )


def whole(shape):
    return pl.BlockSpec(shape, lambda *_: (0,) * len(shape), pipeline_mode=pl.Buffered(1))


def one_hot_rows(code_ref, slots, rows, tile=0):
    slot = lax.broadcasted_iota(i32, (slots, rows), 0) + tile * slots
    picks = (slot == code_ref[0:1, :]) | (slot == code_ref[1:2, :])
    return jnp.where(picks, 1.0, 0.0).astype(bf16)


def spread_gain(gain_ref, wide_ref):
    lanes = gain_ref.shape[1]
    gain = gain_ref[...].astype(f32)
    for k in range(gain_ref.shape[0]):
        wide_ref[:, k * lanes : (k + 1) * lanes] = gain[k : k + 1, :]


def near_body(q_ref, code_ref, x_ref, gain_ref, out_ref, factor_ref, normed_ref, wide_ref, *, quarter, half):
    step = pl.program_id(0)
    block, width = x_ref.shape
    side = out_ref.shape[1]

    @pl.when(step == 0)
    def _():
        spread_gain(gain_ref, wide_ref)

    @pl.when(step < half)
    def _():
        x = x_ref[...].astype(f32)
        factor = lax.rsqrt(jnp.sum(x * x, axis=1, keepdims=True) / width + 1e-06)
        factor_ref[...] = jnp.broadcast_to(factor, factor_ref.shape)
        columns = pl.ds(pl.multiple_of(q_ref[0] * quarter, quarter), side)
        piece = x_ref[:, columns].astype(f32) * factor * wide_ref[:, columns]
        normed_ref[pl.ds(step * block, block), :] = piece.astype(bf16)

    @pl.when(step >= half)
    def _():
        picks = one_hot_rows(code_ref, out_ref.shape[0], normed_ref.shape[0], step - half)
        out_ref[...] = dot(picks, normed_ref[...]).astype(bf16)


def near_rows(index, code, x, gain, slots, side):
    rows, width = x.shape
    quarter = width // 4
    half = 2
    block, tile = rows // half, slots // half
    return call(
        functools.partial(near_body, quarter=quarter, half=half),
        (2 * half,),
        [
            whole(code.shape),
            pl.BlockSpec((block, width), lambda i, q: (jnp.minimum(i, half - 1), 0)),
            whole(gain.shape),
        ],
        [
            (
                (slots, side),
                bf16,
                pl.BlockSpec((tile, side), lambda i, q: (jnp.maximum(i - half, 0), 0)),
            ),
            (
                (rows, 128),
                f32,
                pl.BlockSpec((block, 128), lambda i, q: (jnp.minimum(i, half - 1), 0)),
            ),
        ],
        [pltpu.VMEM((rows, side), bf16), pltpu.VMEM((1, width), f32)],
        2 * slots * rows * side,
        2 * (rows * width + slots * side),
    )(index, code, x, gain)


def far_body(q_ref, code_ref, x0, x1, x2, x3, gain_ref, factor_ref, out_ref, normed_ref, wide_ref):
    @pl.when(pl.program_id(0) == 0)
    def _():
        spread_gain(gain_ref, wide_ref)
        quarter, rest = x0.shape[1], x1.shape[1]
        at = 0
        for x_ref, step in ((x0, 2), (x1, 0), (x2, 1), (x3, 3)):
            size = x_ref.shape[1]
            start = (q_ref[0] + step) % 4 * quarter + quarter - size
            gain = wide_ref[:, pl.ds(pl.multiple_of(start, rest), size)]
            piece = x_ref[...].astype(f32) * factor_ref[:, 0:1] * gain
            normed_ref[:, at : at + size] = piece.astype(bf16)
            at += size

    picks = one_hot_rows(code_ref, out_ref.shape[0], normed_ref.shape[0], pl.program_id(0))
    out_ref[...] = dot(picks, normed_ref[...]).astype(bf16)


def far_rows(index, code, x, gain, factor, slots, side):
    rows, width = x.shape
    quarter = width // 4
    rest = quarter - side
    each = quarter // rest
    total = quarter + 3 * rest
    steps = 4

    def last(step):
        return (rest, lambda i, q: (0, (q[0] + step) % 4 * each + each - 1))

    places = [(quarter, lambda i, q: (0, (q[0] + 2) % 4)), last(0), last(1), last(3)]
    once = pl.Buffered(1)
    return call(
        far_body,
        (steps,),
        [whole(code.shape)]
        + [pl.BlockSpec((rows, size), place, pipeline_mode=once) for size, place in places]
        + [whole(gain.shape), whole(factor.shape)],
        [((slots, total), bf16, pl.BlockSpec((slots // steps, total), lambda i, q: (i, 0)))],
        [pltpu.VMEM((rows, total), bf16), pltpu.VMEM((1, width), f32)],
        2 * slots * rows * total,
        2 * (rows + slots) * total,
    )(index, code, x, x, x, x, gain, factor)[0]


def lent_block(rows, units, quarter, step):
    return pl.BlockSpec(
        (pl.Element(rows), pl.Element(units)),
        lambda i, q: ((q[0] + step) % 4 * quarter, 0),
        pipeline_mode=pl.Buffered(1),
    )


def first_body(q_ref, near_ref, wg_ref, wu_ref, gate_ref, up_ref):
    gate_ref[...] = dot(near_ref[...], wg_ref[...])
    up_ref[...] = dot(near_ref[...], wu_ref[...])


def first_part(index, near, wg, wu):
    slots, side = near.shape
    units = wg.shape[1]
    quarter = wg.shape[0] // 4
    steps = 4
    tile = slots // steps
    rowed = pl.BlockSpec((tile, units), lambda i, q: (i, 0))
    return call(
        first_body,
        (steps,),
        [pl.BlockSpec((tile, side), lambda i, q: (i, 0))] + [lent_block(side, units, quarter, 0)] * 2,
        [((slots, units), f32, rowed), ((slots, units), f32, rowed)],
        (),
        4 * slots * side * units,
        2 * slots * side + 4 * side * units + 8 * slots * units,
    )(index, near, wg, wu)


def second_body(q_ref, right_ref, left_ref, gate_ref, up_ref, gr, gl, ur, ul, gate_out, up_out):
    right, left = right_ref[...], left_ref[...]
    gate_out[...] = gate_ref[...] + dot(right, gr[...]) + dot(left, gl[...])
    up_out[...] = up_ref[...] + dot(right, ur[...]) + dot(left, ul[...])


def second_part(index, right, left, gate, up, wg, wu):
    early, side = right.shape
    units = wg.shape[1]
    quarter = wg.shape[0] // 4
    steps = 3
    tile = early // steps
    rowed = pl.BlockSpec((tile, units), lambda i, q: (i, 0))
    lent = pl.BlockSpec((tile, side), lambda i, q: (i, 0))
    weights = [lent_block(side, units, quarter, step) for step in (1, 3)]
    return call(
        second_body,
        (steps,),
        [lent, lent, rowed, rowed] + weights * 2,
        [((early, units), f32, rowed), ((early, units), f32, rowed)],
        (),
        8 * early * side * units,
        4 * early * side + 8 * side * units + 16 * early * units,
    )(index, right, left, gate, up, wg, wg, wu, wu)


def hidden_body(
    q_ref,
    far_ref,
    right_ref,
    left_ref,
    gate_ref,
    up_ref,
    last_gate,
    last_up,
    wg_ref,
    wu_ref,
    out_ref,
    both_ref,
    far_weight,
    lent_weight,
    sems,
    *,
    capacity,
):
    step, last = pl.program_id(0), pl.num_programs(0) - 1
    parts, count, units = out_ref.shape
    size = parts * count
    side = right_ref.shape[1]
    quarter = wg_ref.shape[0] // 4
    rest = quarter - side

    def copies(weight, segments, first):
        made, at = [], 0
        for turn, skip, rows in segments:
            start = pl.multiple_of((q_ref[0] + turn) % 4 * quarter + skip, rest)
            for k, ref in enumerate((wg_ref, wu_ref)):
                made.append(
                    pltpu.make_async_copy(
                        ref.at[pl.ds(start, rows), :],
                        weight.at[pl.ds(at, rows), pl.ds(k * units, units)],
                        sems.at[first + len(made)],
                    )
                )
            at += rows
        return made

    far_copies = copies(
        far_weight, ((2, 0, quarter), (0, side, rest), (1, side, rest), (3, side, rest)), 0
    )
    lent_copies = copies(lent_weight, ((1, 0, side), (3, 0, side)), len(far_copies))

    @pl.when(step == 0)
    def _():
        for copy in far_copies + lent_copies:
            copy.start()
        for copy in far_copies:
            copy.wait()

    both_ref[...] = dot(far_ref[...], far_weight[...])

    @pl.when(step < last)
    def _():
        both_ref[:, :units] += gate_ref[...]
        both_ref[:, units:] += up_ref[...]

    @pl.when(step == last)
    def _():
        for copy in lent_copies:
            copy.wait()
        both_ref[...] += dot(right_ref[...], lent_weight[:side, :])
        both_ref[...] += dot(left_ref[...], lent_weight[side:, :])
        both_ref[:, :units] += last_gate[...]
        both_ref[:, units:] += last_up[...]

    gate = both_ref[:, :units]
    hidden = (gate / (1.0 + jnp.exp(-gate)) * both_ref[:, units:]).astype(bf16)
    row = lax.broadcasted_iota(i32, (size, 1), 0)
    place = row % count // capacity * (parts * capacity) + row // count * capacity + row % capacity
    column = lax.broadcasted_iota(i32, (size, size), 1)
    order = jnp.where(column == place, 1.0, 0.0).astype(bf16)
    out_ref[...] = dot(order, hidden).astype(bf16).reshape(parts, count, units)


def hidden_units(index, far, right, left, sums, starts, wg, wu, capacity):
    slots, depth = far.shape
    tile, side = right.shape
    units = wg.shape[1]
    steps, parts = slots // tile, 4
    once = pl.Buffered(1)
    early = pl.BlockSpec((tile, units), lambda i, q: (jnp.minimum(i, steps - 2), 0))
    late = pl.BlockSpec((tile, units), lambda i, q: (steps - 1, 0), pipeline_mode=once)
    place = pl.BlockSpec(memory_space=pl.ANY)
    return call(
        functools.partial(hidden_body, capacity=capacity),
        (steps,),
        [
            pl.BlockSpec((tile, depth), lambda i, q: (i, 0)),
            whole(right.shape),
            whole(left.shape),
            early,
            early,
            late,
            late,
            place,
            place,
        ],
        [
            (
                (parts, slots // parts, units),
                bf16,
                pl.BlockSpec((parts, tile // parts, units), lambda i, q: (0, i, 0)),
            )
        ],
        [
            pltpu.VMEM((tile, 2 * units), f32),
            pltpu.VMEM((depth, 2 * units), bf16),
            pltpu.VMEM((2 * side, 2 * units), bf16),
            pltpu.SemaphoreType.DMA((12,)),
        ],
        4 * slots * depth * units + 8 * tile * side * units,
        2 * slots * depth + 4 * depth * units + 10 * slots * units,
    )(index, far, right, left, *sums, *starts, wg, wu)[0]


def rows_of(hidden, step):
    parts, count, units = hidden.shape
    return pl.BlockSpec(
        (None, count, units), lambda i, q: ((q[0] + step) % parts, 0, 0), pipeline_mode=pl.Buffered(1)
    )


def sides_body(q_ref, to_right_ref, to_left_ref, down_ref, right_ref, left_ref):
    count = to_right_ref.shape[0]
    value = dot(jnp.concatenate([to_right_ref[...], to_left_ref[...]], axis=0), down_ref[...])
    right_ref[...] = value[:count].astype(bf16)
    left_ref[...] = value[count:].astype(bf16)


def side_rows(index, hidden, down, piece, pieces):
    _, count, units = hidden.shape
    width = down.shape[1] // pieces
    steps = 2
    tile = width // steps
    tiled = pl.BlockSpec((count, tile), lambda i, q: (0, i))
    return call(
        sides_body,
        (steps,),
        [
            rows_of(hidden, 1),
            rows_of(hidden, 3),
            pl.BlockSpec((units, tile), lambda i, q: (0, piece * steps + i)),
        ],
        [((count, width), bf16, tiled), ((count, width), bf16, tiled)],
        (),
        4 * count * units * width,
        2 * (2 * count * units + units * width + 2 * count * width),
    )(index, hidden, hidden, down)


def own_body(q_ref, rows_ref, down_ref, out_ref):
    out_ref[...] = dot(rows_ref[...], down_ref[...]).astype(bf16)


def own_rows(index, hidden, down, piece, pieces):
    _, count, units = hidden.shape
    width = down.shape[1] // pieces
    steps = 2
    tile = width // steps
    return call(
        own_body,
        (steps,),
        [rows_of(hidden, 0)]
        + [pl.BlockSpec((units, tile), lambda i, q: (0, piece * steps + i))],
        [((count, width), bf16, pl.BlockSpec((count, tile), lambda i, q: (0, i)))],
        (),
        2 * count * units * width,
        2 * (count * units + units * width + count * width),
    )(index, hidden, down)[0]


def order_of(many, capacity, parts):
    size, each = many * parts, parts * capacity
    row = lax.broadcasted_iota(i32, (size, 1), 0)
    place = row % each // capacity * many + row // each * capacity + row % capacity
    column = lax.broadcasted_iota(i32, (size, size), 1)
    return jnp.where(column == place, 1.0, 0.0).astype(bf16)


def messages_of(order, value, fold, parts):
    stack = jnp.concatenate([value[:, k * fold : (k + 1) * fold] for k in range(parts)], axis=0)
    return dot(order, stack).astype(bf16)


def across_body(q_ref, rows_ref, down_ref, out_ref, value_ref, *, capacity, parts, steps):
    step = pl.program_id(0)
    tile, fold = down_ref.shape[1], out_ref.shape[1]
    groups = 2
    many = out_ref.shape[0] // (parts * groups)

    @pl.when(step < steps)
    def _():
        columns = pl.ds(pl.multiple_of(step * tile, tile), tile)
        value_ref[:, columns] = dot(rows_ref[...], down_ref[...]).astype(bf16)

    @pl.when(step >= steps)
    def _():
        order = order_of(many, capacity, parts)
        size = many * parts
        for g in range(groups):
            start = pl.multiple_of(((step - steps) * groups + g) * many, many)
            value = value_ref[pl.ds(start, many), :]
            out_ref[g * size : (g + 1) * size, :] = messages_of(order, value, fold, parts)


def across_messages(index, hidden, down, capacity):
    parts, count, units = hidden.shape
    width = down.shape[1]
    slots, fold = parts * count, width // parts
    steps = 2
    tile = width // steps
    return call(
        functools.partial(across_body, capacity=capacity, parts=parts, steps=steps),
        (2 * steps,),
        [rows_of(hidden, 2)]
        + [pl.BlockSpec((units, tile), lambda i, q: (0, jnp.minimum(i, steps - 1)))],
        [
            (
                (slots, fold),
                bf16,
                pl.BlockSpec((slots // steps, fold), lambda i, q: (jnp.maximum(i - steps, 0), 0)),
            )
        ],
        [pltpu.VMEM((count, width), bf16)],
        2 * count * units * width,
        2 * (count * units + units * width + count * width),
    )(index, hidden, down)[0]


def summed_body(q_ref, own_ref, left_ref, right_ref, out_ref, *, capacity, parts):
    groups = 2
    fold = out_ref.shape[1]
    size = out_ref.shape[0] // groups
    many = size // parts
    order = order_of(many, capacity, parts)
    for g in range(groups):
        part = slice(g * many, (g + 1) * many)
        total = own_ref[part, :].astype(f32) + left_ref[part, :].astype(f32)
        total = (total + right_ref[part, :].astype(f32)).astype(bf16)
        out_ref[g * size : (g + 1) * size, :] = messages_of(order, total, fold, parts)


def summed_messages(index, own, left, right, capacity, parts):
    count, width = own.shape
    slots, fold = count * parts, width // parts
    steps = 2
    rowed = pl.BlockSpec((count // steps, width), lambda i, q: (i, 0))
    return call(
        functools.partial(summed_body, capacity=capacity, parts=parts),
        (steps,),
        [rowed, rowed, rowed],
        [((slots, fold), bf16, pl.BlockSpec((slots // steps, fold), lambda i, q: (i, 0)))],
        (),
        2 * slots * slots // 4 * fold,
        8 * count * width,
    )(index, own, left, right)[0]


def combine_body(q_ref, home_ref, share_ref, rows_ref, *refs, capacity, parts):
    out_ref, weight_ref, value_ref = refs[-3:]
    extra = refs[0] if len(refs) > 3 else None
    step = pl.program_id(0)
    slots, tile = rows_ref.shape
    block, width = out_ref.shape

    @pl.when(step == 0)
    def _():
        column = lax.broadcasted_iota(i32, (block, slots), 1)
        for k in range(parts):
            home = home_ref[...] + k * capacity
            weights = jnp.where(column == home[:, 0:1], share_ref[:, 0:1], 0.0)
            weights = jnp.where(column == home[:, 1:2], share_ref[:, 1:2], weights)
            weight_ref[k * block : (k + 1) * block, :] = weights.astype(bf16)

    value_ref[...] = dot(weight_ref[...], rows_ref[...])
    for k in range(parts):
        columns = pl.ds(pl.multiple_of(k * (width // parts) + step * tile, tile), tile)
        value = value_ref[k * block : (k + 1) * block, :]
        if extra is not None:
            value = value + extra[:, columns].astype(f32)
        out_ref[:, columns] = value.astype(bf16)


def combined(index, home, share, rows, capacity, parts, extra=None, into=None, piece=0, pieces=1):
    slots, fold = rows.shape
    block = home.shape[0]
    width = parts * fold
    steps = 2
    placed = pl.BlockSpec((block, width), lambda i, q: (0, piece), pipeline_mode=pl.Buffered(1))
    ins = [
        whole(home.shape),
        whole(share.shape),
        pl.BlockSpec((slots, fold // steps), lambda i, q: (0, i)),
    ]
    args = [home, share, rows]
    if extra is not None:
        ins.append(placed)
        args.append(extra)
    if into is not None:
        ins.append(pl.BlockSpec(memory_space=pl.ANY))
        args.append(into)
    return pl.pallas_call(
        functools.partial(combine_body, capacity=capacity, parts=parts),
        out_shape=jax.ShapeDtypeStruct((block, width * pieces), bf16),
        grid_spec=pltpu.PrefetchScalarGridSpec(
            num_scalar_prefetch=1,
            grid=(steps,),
            in_specs=ins,
            out_specs=placed,
            scratch_shapes=[
                pltpu.VMEM((parts * block, slots), bf16),
                pltpu.VMEM((parts * block, fold // steps), f32),
            ],
        ),
        input_output_aliases={} if into is None else {len(args): 0},
        cost_estimate=pl.CostEstimate(
            flops=2 * parts * block * slots * fold,
            bytes_accessed=2 * slots * fold + 4 * block * width,
            transcendentals=0,
        ),
        name="combined",
    )(index, *args)


def mixed_body(q_ref, hidden_ref, weight_ref, own_ref, *outs):
    step = pl.program_id(0)
    parts = 4
    block = own_ref.shape[0]
    middle = pl.num_programs(0) // 2

    def rows_for(which):
        start = pl.multiple_of((q_ref[0] + which) % parts * block, block)
        return dot(hidden_ref[pl.ds(start, block), :], weight_ref[...]).astype(bf16)

    own_ref[...] = rows_for(0)

    @pl.when(step < middle)
    def _():
        for k in range(parts - 1):
            outs[2 * k][...] = rows_for(k + 1)

    @pl.when(step >= middle)
    def _():
        for k in range(parts - 1):
            outs[2 * k + 1][...] = rows_for(k + 1)


def mixed_rows(index, hidden, weight, parts):
    rows, channels = hidden.shape
    width = weight.shape[1]
    steps = 4
    block, tile = rows // parts, width // steps
    low = pl.BlockSpec((block, tile), lambda i, q: (0, jnp.minimum(i, steps // 2 - 1)))
    high = pl.BlockSpec((block, tile), lambda i, q: (0, jnp.maximum(i - steps // 2, 0)))
    return call(
        mixed_body,
        (steps,),
        [whole(hidden.shape), pl.BlockSpec((channels, tile), lambda i, q: (0, i))],
        [((block, width), bf16, pl.BlockSpec((block, tile), lambda i, q: (0, i)))]
        + [((block, width // 2), bf16, low), ((block, width // 2), bf16, high)] * (parts - 1),
        (),
        2 * rows * channels * width,
        2 * (rows * channels + channels * width + rows * width),
    )(index, hidden, weight)


def on_device(
    mixer_value,
    mixer_gate,
    mixer_taps,
    mixer_gain,
    mixer_weight,
    routed_input,
    routed_gain,
    expert_ids,
    route_share,
    gate_weight,
    up_weight,
    down_weight,
):
    parts = lax.axis_size("tp")
    sources = lax.axis_size("ep")
    q = lax.axis_index("tp").astype(i32)
    index = q.reshape(1)
    across = (q + 2) % parts
    rows, width = routed_input.shape
    block = rows // parts
    chosen = expert_ids.shape[1]
    capacity = 5 * block // (2 * sources)
    per_source = parts * capacity
    slots = sources * per_source
    quarter = width // parts
    side = 7 * quarter // 8
    early = 3 * slots // 4

    ids = expert_ids.T.reshape(chosen, parts, block)
    earlier = jnp.arange(block)[:, None] < jnp.arange(block)[None, :]
    same = ids[:, None, :, :, None] == ids[None, :, :, None, :]
    rank = jnp.sum((same & earlier).astype(i32), axis=(0, 3))
    code = ids * per_source + jnp.arange(parts, dtype=i32)[None, :, None] * capacity + rank
    code = code.reshape(chosen, rows)

    def exchanged(messages):
        size = messages.shape[1]
        messages = messages.reshape(sources, per_source, size)
        return lax.all_to_all(messages, "ep", 0, 0, tiled=True).reshape(slots, size)

    taps = mixer_taps.shape[0]
    length = mixer_value.shape[0]
    last_value, last_gate = mixer_value[length - (taps - 1) :], mixer_gate[length - (taps - 1) :]
    last = (last_value.astype(f32) * jax.nn.sigmoid(last_gate.astype(f32))).astype(bf16)
    before = lax.ppermute(last, "ep", [(i, i + 1) for i in range(sources - 1)])

    gain = routed_gain.reshape(-1, 128)
    near, factor = near_rows(index, code, routed_input, gain, slots, side)
    near, before, mixer_value, mixer_gate, mixer_taps = lax.optimization_barrier(
        (near, before, mixer_value, mixer_gate, mixer_taps)
    )
    near = exchanged(near)
    gated = (mixer_value.astype(f32) * jax.nn.sigmoid(mixer_gate.astype(f32))).astype(bf16)

    extended = jnp.concatenate([before, gated], axis=0).astype(f32)
    taps_float = mixer_taps.astype(f32)
    filtered = taps_float[0] * extended[0:length]
    for offset in range(1, taps):
        filtered = filtered + taps_float[offset] * extended[offset : offset + length]
    stats = jnp.stack([jnp.sum(filtered, axis=1), jnp.sum(filtered * filtered, axis=1)])
    stats = stats + turned(stats, "tp", 1) + turned(stats, "tp", -1) + turned(stats, "tp", 2)
    channels = mixer_taps.shape[1] * parts
    center = stats[0] / channels
    spread = stats[1] / channels - center * center
    normed_mix = (
        (filtered - center[:, None])
        * lax.rsqrt(spread + 1e-05)[:, None]
        * mixer_gain.astype(f32)
    )
    mixer_hidden = jax.nn.silu(normed_mix).astype(bf16)
    mix_own, right_low, right_high, far_low, far_high, left_low, left_high = mixed_rows(
        index, mixer_hidden, mixer_weight, parts
    )
    via_right, via_left = turned(far_low, "tp", 1), turned(far_high, "tp", -1)
    raw_high, raw_low = turned(right_high, "tp", 1), turned(left_low, "tp", -1)

    factor, right_low, left_high = lax.optimization_barrier((factor, right_low, left_high))
    far = far_rows(index, code, routed_input, gain, factor, slots, side)
    lent = []
    for piece in (near[:early], near[early:]):
        lent.append((turned(piece, "tp", -1), turned(piece, "tp", 1)))
    far = exchanged(far)

    sum_low = turned((right_low.astype(f32) + via_right.astype(f32)).astype(bf16), "tp", 1)
    sum_high = turned((left_high.astype(f32) + via_left.astype(f32)).astype(bf16), "tp", -1)
    middle = width // 2
    mixer_result = jnp.concatenate(
        [
            mix_own[:, :middle].astype(f32) + sum_low.astype(f32) + raw_low.astype(f32),
            mix_own[:, middle:].astype(f32) + sum_high.astype(f32) + raw_high.astype(f32),
        ],
        axis=1,
    ).astype(bf16)

    weights = (gate_weight[0], up_weight[0])

    starts = first_part(index, near, *weights)
    sums = second_part(index, *lent[0], *starts, *weights)
    hidden = hidden_units(index, far, *lent[1], sums, starts, *weights, capacity)

    def home_of(which):
        own_ids = lax.dynamic_slice_in_dim(ids, which, 1, 1)[:, 0]
        own_rank = lax.dynamic_slice_in_dim(rank, which, 1, 1)[:, 0]
        own_share = lax.dynamic_slice_in_dim(route_share, which * block, block, 0)
        return (own_ids * per_source + own_rank).T, own_share

    down = down_weight[0]
    far_home, own_home = home_of(across), home_of(q)
    got = []
    for piece in range(PIECES):
        to_right, to_left = side_rows(index, hidden, down, piece, PIECES)
        got.append((turned(to_right, "tp", 1), turned(to_left, "tp", -1)))
    messages = across_messages(index, hidden, down, capacity)
    far_back = exchanged(messages)
    own = [own_rows(index, hidden, down, piece, PIECES) for piece in range(PIECES)]
    extra = combined(index, *far_home, far_back, capacity, parts)
    extra, own[-1] = lax.optimization_barrier((extra, own[-1]))
    extra = turned(extra, "tp", 2)
    result = None
    for piece in range(PIECES):
        messages = summed_messages(index, own[piece], *got[piece], capacity, parts)
        back = exchanged(messages)
        result = combined(index, *own_home, back, capacity, parts, extra, result, piece, PIECES)
    return (mixer_result, result)


def solution(mesh):
    return jax.shard_map(
        on_device,
        mesh=mesh,
        in_specs=(
            P("ep", "tp"),
            P("ep", "tp"),
            P(None, "tp"),
            P("tp"),
            P("tp", None),
            P("ep", None),
            P(),
            P("ep", None),
            P("ep", None),
            P("ep", None, "tp"),
            P("ep", None, "tp"),
            P("ep", "tp", None),
        ),
        out_specs=(P(("ep", "tp"), None), P(("ep", "tp"), None)),
        check_vma=False,
    )
```

```python
import functools

import jax
import jax.numpy as jnp
from jax import lax
from jax.experimental import pallas as pl
from jax.experimental.pallas import tpu as pltpu
from jax.sharding import PartitionSpec as P


PIECES = 2
f32 = jnp.float32
bf16 = jnp.bfloat16
i32 = jnp.int32


def turned(value, axis, steps):
    count = lax.axis_size(axis)
    return lax.ppermute(value, axis, [(i, (i + steps) % count) for i in range(count)])


def dot(a, b):
    return jnp.dot(a, b, preferred_element_type=f32)


LIMITS = {
    "own_rows": 8,
    "summed_messages": 8,
    "combined": 12,
}


def limited(name):
    if name not in LIMITS:
        return None
    return pltpu.CompilerParams(vmem_limit_bytes=LIMITS[name] * 1024 * 1024)


def call(body, name, grid, ins, outs, scratch=(), flops=0, moved=0, prefetch=1):
    return pl.pallas_call(
        body,
        out_shape=[jax.ShapeDtypeStruct(shape, kind) for shape, kind, _ in outs],
        grid_spec=pltpu.PrefetchScalarGridSpec(
            num_scalar_prefetch=prefetch,
            grid=grid,
            in_specs=ins,
            out_specs=[spec for _, _, spec in outs],
            scratch_shapes=list(scratch),
        ),
        cost_estimate=pl.CostEstimate(flops=flops, bytes_accessed=moved, transcendentals=0),
        compiler_params=limited(name),
    )


def whole(shape):
    return pl.BlockSpec(shape, lambda *_: (0,) * len(shape), pipeline_mode=pl.Buffered(1))


def one_hot_rows(code_ref, slots, rows, tile=0):
    slot = lax.broadcasted_iota(i32, (slots, rows), 0) + tile * slots
    picks = (slot == code_ref[0:1, :]) | (slot == code_ref[1:2, :])
    return jnp.where(picks, 1.0, 0.0).astype(bf16)


def spread_gain(gain_ref, wide_ref):
    lanes = gain_ref.shape[1]
    gain = gain_ref[...].astype(f32)
    for k in range(gain_ref.shape[0]):
        wide_ref[:, k * lanes : (k + 1) * lanes] = gain[k : k + 1, :]


def write_codes(ids_ref, code_ref, parts, experts, capacity):
    chosen, rows = ids_ref.shape
    block = rows // parts
    expert = lax.broadcasted_iota(i32, (experts, block), 0)
    earlier = lax.broadcasted_iota(i32, (block, block), 0)
    earlier = jnp.where(earlier < lax.broadcasted_iota(i32, (block, block), 1), 1.0, 0.0)
    for b in range(parts):
        lanes = slice(b * block, (b + 1) * block)
        named = [jnp.where(expert == ids_ref[c : c + 1, lanes], 1.0, 0.0) for c in range(chosen)]
        before = dot((named[0] + named[1]).astype(bf16), earlier.astype(bf16))
        for c in range(chosen):
            rank = jnp.sum(named[c] * before, axis=0, keepdims=True).astype(i32)
            place = ids_ref[c : c + 1, lanes] * (parts * capacity) + (b * capacity)
            code_ref[c : c + 1, lanes] = place + rank


def near_body(
    q_ref,
    ids_ref,
    x_ref,
    gain_ref,
    out_ref,
    factor_ref,
    code_ref,
    normed_ref,
    wide_ref,
    *,
    half,
    experts,
    capacity,
):
    step = pl.program_id(0)
    block, width = x_ref.shape
    parts = 4
    quarter = width // parts
    side = out_ref.shape[1]

    @pl.when(step == 0)
    def _():
        spread_gain(gain_ref, wide_ref)
        write_codes(ids_ref, code_ref, parts, experts, capacity)

    @pl.when(step < half)
    def _():
        x = x_ref[...].astype(f32)
        factor = lax.rsqrt(jnp.sum(x * x, axis=1, keepdims=True) / width + 1e-06)
        factor_ref[...] = jnp.broadcast_to(factor, factor_ref.shape)
        columns = pl.ds(pl.multiple_of(q_ref[0] * quarter, quarter), side)
        piece = x_ref[:, columns].astype(f32) * factor * wide_ref[:, columns]
        normed_ref[pl.ds(step * block, block), :] = piece.astype(bf16)

    @pl.when(step >= half)
    def _():
        picks = one_hot_rows(code_ref, out_ref.shape[0], normed_ref.shape[0], step - half)
        out_ref[...] = dot(picks, normed_ref[...]).astype(bf16)


def near_rows(index, ids, x, gain, slots, side, experts, capacity):
    rows, width = x.shape
    half = 2
    block, tile = rows // half, slots // half
    return call(
        functools.partial(near_body, half=half, experts=experts, capacity=capacity),
        "near_rows",
        (2 * half,),
        [
            whole(ids.shape),
            pl.BlockSpec((block, width), lambda i, q: (jnp.minimum(i, half - 1), 0)),
            whole(gain.shape),
        ],
        [
            (
                (slots, side),
                bf16,
                pl.BlockSpec((tile, side), lambda i, q: (jnp.maximum(i - half, 0), 0)),
            ),
            (
                (rows, 128),
                f32,
                pl.BlockSpec((block, 128), lambda i, q: (jnp.minimum(i, half - 1), 0)),
            ),
            (ids.shape, i32, whole(ids.shape)),
        ],
        [pltpu.VMEM((rows, side), bf16), pltpu.VMEM((1, width), f32)],
        2 * slots * rows * side,
        2 * (rows * width + slots * side),
    )(index, ids, x, gain)


def far_body(q_ref, code_ref, x0, x1, x2, x3, gain_ref, factor_ref, out_ref, normed_ref, wide_ref):
    @pl.when(pl.program_id(0) == 0)
    def _():
        spread_gain(gain_ref, wide_ref)
        quarter, rest = x0.shape[1], x1.shape[1]
        at = 0
        for x_ref, step in ((x0, 2), (x1, 0), (x2, 1), (x3, 3)):
            size = x_ref.shape[1]
            start = (q_ref[0] + step) % 4 * quarter + quarter - size
            gain = wide_ref[:, pl.ds(pl.multiple_of(start, rest), size)]
            piece = x_ref[...].astype(f32) * factor_ref[:, 0:1] * gain
            normed_ref[:, at : at + size] = piece.astype(bf16)
            at += size

    picks = one_hot_rows(code_ref, out_ref.shape[0], normed_ref.shape[0], pl.program_id(0))
    out_ref[...] = dot(picks, normed_ref[...]).astype(bf16)


def far_rows(index, code, x, gain, factor, slots, side):
    rows, width = x.shape
    quarter = width // 4
    rest = quarter - side
    each = quarter // rest
    total = quarter + 3 * rest
    steps = 4

    def last(step):
        return (rest, lambda i, q: (0, (q[0] + step) % 4 * each + each - 1))

    places = [(quarter, lambda i, q: (0, (q[0] + 2) % 4)), last(0), last(1), last(3)]
    once = pl.Buffered(1)
    return call(
        far_body,
        "far_rows",
        (steps,),
        [whole(code.shape)]
        + [pl.BlockSpec((rows, size), place, pipeline_mode=once) for size, place in places]
        + [whole(gain.shape), whole(factor.shape)],
        [((slots, total), bf16, pl.BlockSpec((slots // steps, total), lambda i, q: (i, 0)))],
        [pltpu.VMEM((rows, total), bf16), pltpu.VMEM((1, width), f32)],
        2 * slots * rows * total,
        2 * (rows + slots) * total,
    )(index, code, x, x, x, x, gain, factor)[0]


def lent_block(rows, units, quarter, step):
    return pl.BlockSpec(
        (pl.Element(rows), pl.Element(units)),
        lambda i, q: ((q[0] + step) % 4 * quarter, 0),
        pipeline_mode=pl.Buffered(1),
    )


def first_body(q_ref, near_ref, wg_ref, wu_ref, gate_ref, up_ref):
    gate_ref[...] = dot(near_ref[...], wg_ref[...])
    up_ref[...] = dot(near_ref[...], wu_ref[...])


def first_part(index, near, wg, wu):
    slots, side = near.shape
    units = wg.shape[1]
    quarter = wg.shape[0] // 4
    steps = 4
    tile = slots // steps
    rowed = pl.BlockSpec((tile, units), lambda i, q: (i, 0))
    return call(
        first_body,
        "first_part",
        (steps,),
        [pl.BlockSpec((tile, side), lambda i, q: (i, 0))] + [lent_block(side, units, quarter, 0)] * 2,
        [((slots, units), f32, rowed), ((slots, units), f32, rowed)],
        (),
        4 * slots * side * units,
        2 * slots * side + 4 * side * units + 8 * slots * units,
    )(index, near, wg, wu)


def second_body(q_ref, right_ref, left_ref, gate_ref, up_ref, gr, gl, ur, ul, gate_out, up_out):
    right, left = right_ref[...], left_ref[...]
    gate_out[...] = gate_ref[...] + dot(right, gr[...]) + dot(left, gl[...])
    up_out[...] = up_ref[...] + dot(right, ur[...]) + dot(left, ul[...])


def second_part(index, right, left, gate, up, wg, wu):
    early, side = right.shape
    units = wg.shape[1]
    quarter = wg.shape[0] // 4
    steps = 3
    tile = early // steps
    rowed = pl.BlockSpec((tile, units), lambda i, q: (i, 0))
    lent = pl.BlockSpec((tile, side), lambda i, q: (i, 0))
    weights = [lent_block(side, units, quarter, step) for step in (1, 3)]
    return call(
        second_body,
        "second_part",
        (steps,),
        [lent, lent, rowed, rowed] + weights * 2,
        [((early, units), f32, rowed), ((early, units), f32, rowed)],
        (),
        8 * early * side * units,
        4 * early * side + 8 * side * units + 16 * early * units,
    )(index, right, left, gate, up, wg, wg, wu, wu)


def hidden_body(
    q_ref,
    far_ref,
    right_ref,
    left_ref,
    gate_ref,
    up_ref,
    last_gate,
    last_up,
    wg_ref,
    wu_ref,
    out_ref,
    both_ref,
    far_weight,
    lent_weight,
    sems,
    *,
    capacity,
):
    step, last = pl.program_id(0), pl.num_programs(0) - 1
    parts, count, units = out_ref.shape
    size = parts * count
    side = right_ref.shape[1]
    quarter = wg_ref.shape[0] // 4
    rest = quarter - side

    def copies(weight, segments, first):
        made, at = [], 0
        for turn, skip, rows in segments:
            start = pl.multiple_of((q_ref[0] + turn) % 4 * quarter + skip, rest)
            for k, ref in enumerate((wg_ref, wu_ref)):
                made.append(
                    pltpu.make_async_copy(
                        ref.at[pl.ds(start, rows), :],
                        weight.at[pl.ds(at, rows), pl.ds(k * units, units)],
                        sems.at[first + len(made)],
                    )
                )
            at += rows
        return made

    far_copies = copies(
        far_weight, ((2, 0, quarter), (0, side, rest), (1, side, rest), (3, side, rest)), 0
    )
    lent_copies = copies(lent_weight, ((1, 0, side), (3, 0, side)), len(far_copies))

    @pl.when(step == 0)
    def _():
        for copy in far_copies + lent_copies:
            copy.start()
        for copy in far_copies:
            copy.wait()

    both_ref[...] = dot(far_ref[...], far_weight[...])

    @pl.when(step < last)
    def _():
        both_ref[:, :units] += gate_ref[...]
        both_ref[:, units:] += up_ref[...]

    @pl.when(step == last)
    def _():
        for copy in lent_copies:
            copy.wait()
        both_ref[...] += dot(right_ref[...], lent_weight[:side, :])
        both_ref[...] += dot(left_ref[...], lent_weight[side:, :])
        both_ref[:, :units] += last_gate[...]
        both_ref[:, units:] += last_up[...]

    gate = both_ref[:, :units]
    hidden = (gate / (1.0 + jnp.exp(-gate)) * both_ref[:, units:]).astype(bf16)
    row = lax.broadcasted_iota(i32, (size, 1), 0)
    place = row % count // capacity * (parts * capacity) + row // count * capacity + row % capacity
    column = lax.broadcasted_iota(i32, (size, size), 1)
    order = jnp.where(column == place, 1.0, 0.0).astype(bf16)
    out_ref[...] = dot(order, hidden).astype(bf16).reshape(parts, count, units)


def hidden_units(index, far, right, left, sums, starts, wg, wu, capacity):
    slots, depth = far.shape
    tile, side = right.shape
    units = wg.shape[1]
    steps, parts = slots // tile, 4
    once = pl.Buffered(1)
    early = pl.BlockSpec((tile, units), lambda i, q: (jnp.minimum(i, steps - 2), 0))
    late = pl.BlockSpec((tile, units), lambda i, q: (steps - 1, 0), pipeline_mode=once)
    place = pl.BlockSpec(memory_space=pl.ANY)
    return call(
        functools.partial(hidden_body, capacity=capacity),
        "hidden_units",
        (steps,),
        [
            pl.BlockSpec((tile, depth), lambda i, q: (i, 0)),
            whole(right.shape),
            whole(left.shape),
            early,
            early,
            late,
            late,
            place,
            place,
        ],
        [
            (
                (parts, slots // parts, units),
                bf16,
                pl.BlockSpec((parts, tile // parts, units), lambda i, q: (0, i, 0)),
            )
        ],
        [
            pltpu.VMEM((tile, 2 * units), f32),
            pltpu.VMEM((depth, 2 * units), bf16),
            pltpu.VMEM((2 * side, 2 * units), bf16),
            pltpu.SemaphoreType.DMA((12,)),
        ],
        4 * slots * depth * units + 8 * tile * side * units,
        2 * slots * depth + 4 * depth * units + 10 * slots * units,
    )(index, far, right, left, *sums, *starts, wg, wu)[0]


def rows_of(hidden, step):
    parts, count, units = hidden.shape
    return pl.BlockSpec(
        (None, count, units), lambda i, q: ((q[0] + step) % parts, 0, 0), pipeline_mode=pl.Buffered(1)
    )


def sides_body(q_ref, to_right_ref, to_left_ref, down_ref, right_ref, left_ref):
    count = to_right_ref.shape[0]
    value = dot(jnp.concatenate([to_right_ref[...], to_left_ref[...]], axis=0), down_ref[...])
    right_ref[...] = value[:count].astype(bf16)
    left_ref[...] = value[count:].astype(bf16)


def side_rows(index, hidden, down, piece, pieces):
    _, count, units = hidden.shape
    width = down.shape[1] // pieces
    steps = 2
    tile = width // steps
    tiled = pl.BlockSpec((count, tile), lambda i, q: (0, i))
    return call(
        sides_body,
        "side_rows",
        (steps,),
        [
            rows_of(hidden, 1),
            rows_of(hidden, 3),
            pl.BlockSpec((units, tile), lambda i, q: (0, piece * steps + i)),
        ],
        [((count, width), bf16, tiled), ((count, width), bf16, tiled)],
        (),
        4 * count * units * width,
        2 * (2 * count * units + units * width + 2 * count * width),
    )(index, hidden, hidden, down)


def own_body(q_ref, rows_ref, down_ref, out_ref):
    out_ref[...] = dot(rows_ref[...], down_ref[...]).astype(bf16)


def own_rows(index, hidden, down, piece, pieces):
    _, count, units = hidden.shape
    width = down.shape[1] // pieces
    steps = 2
    tile = width // steps
    return call(
        own_body,
        "own_rows",
        (steps,),
        [rows_of(hidden, 0)]
        + [pl.BlockSpec((units, tile), lambda i, q: (0, piece * steps + i))],
        [((count, width), bf16, pl.BlockSpec((count, tile), lambda i, q: (0, i)))],
        (),
        2 * count * units * width,
        2 * (count * units + units * width + count * width),
    )(index, hidden, down)[0]


def order_of(many, capacity, parts):
    size, each = many * parts, parts * capacity
    row = lax.broadcasted_iota(i32, (size, 1), 0)
    place = row % each // capacity * many + row // each * capacity + row % capacity
    column = lax.broadcasted_iota(i32, (size, size), 1)
    return jnp.where(column == place, 1.0, 0.0).astype(bf16)


def messages_of(order, value, fold, parts):
    stack = jnp.concatenate([value[:, k * fold : (k + 1) * fold] for k in range(parts)], axis=0)
    return dot(order, stack).astype(bf16)


def across_body(q_ref, rows_ref, down_ref, out_ref, value_ref, *, capacity, parts, steps):
    step = pl.program_id(0)
    tile, fold = down_ref.shape[1], out_ref.shape[1]
    groups = 2
    many = out_ref.shape[0] // (parts * groups)

    @pl.when(step < steps)
    def _():
        columns = pl.ds(pl.multiple_of(step * tile, tile), tile)
        value_ref[:, columns] = dot(rows_ref[...], down_ref[...]).astype(bf16)

    @pl.when(step >= steps)
    def _():
        order = order_of(many, capacity, parts)
        size = many * parts
        for g in range(groups):
            start = pl.multiple_of(((step - steps) * groups + g) * many, many)
            value = value_ref[pl.ds(start, many), :]
            out_ref[g * size : (g + 1) * size, :] = messages_of(order, value, fold, parts)


def across_messages(index, hidden, down, capacity):
    parts, count, units = hidden.shape
    width = down.shape[1]
    slots, fold = parts * count, width // parts
    steps = 2
    tile = width // steps
    return call(
        functools.partial(across_body, capacity=capacity, parts=parts, steps=steps),
        "across_messages",
        (2 * steps,),
        [rows_of(hidden, 2)]
        + [pl.BlockSpec((units, tile), lambda i, q: (0, jnp.minimum(i, steps - 1)))],
        [
            (
                (slots, fold),
                bf16,
                pl.BlockSpec((slots // steps, fold), lambda i, q: (jnp.maximum(i - steps, 0), 0)),
            )
        ],
        [pltpu.VMEM((count, width), bf16)],
        2 * count * units * width,
        2 * (count * units + units * width + count * width),
    )(index, hidden, down)[0]


def summed_body(q_ref, own_ref, left_ref, right_ref, out_ref, *, capacity, parts):
    groups = 2
    fold = out_ref.shape[1]
    size = out_ref.shape[0] // groups
    many = size // parts
    order = order_of(many, capacity, parts)
    for g in range(groups):
        part = slice(g * many, (g + 1) * many)
        total = own_ref[part, :].astype(f32) + left_ref[part, :].astype(f32)
        total = (total + right_ref[part, :].astype(f32)).astype(bf16)
        out_ref[g * size : (g + 1) * size, :] = messages_of(order, total, fold, parts)


def summed_messages(index, own, left, right, capacity, parts):
    count, width = own.shape
    slots, fold = count * parts, width // parts
    steps = 2
    rowed = pl.BlockSpec((count // steps, width), lambda i, q: (i, 0))
    return call(
        functools.partial(summed_body, capacity=capacity, parts=parts),
        "summed_messages",
        (steps,),
        [rowed, rowed, rowed],
        [((slots, fold), bf16, pl.BlockSpec((slots // steps, fold), lambda i, q: (i, 0)))],
        (),
        2 * slots * slots // 4 * fold,
        8 * count * width,
    )(index, own, left, right)[0]


def combine_body(q_ref, home_ref, share_ref, rows_ref, *refs, capacity, parts):
    out_ref, weight_ref, value_ref = refs[-3:]
    extra = refs[0] if len(refs) > 3 else None
    step = pl.program_id(0)
    slots, tile = rows_ref.shape
    block, width = out_ref.shape

    @pl.when(step == 0)
    def _():
        column = lax.broadcasted_iota(i32, (block, slots), 1)
        for k in range(parts):
            home = home_ref[...] + k * capacity
            weights = jnp.where(column == home[:, 0:1], share_ref[:, 0:1], 0.0)
            weights = jnp.where(column == home[:, 1:2], share_ref[:, 1:2], weights)
            weight_ref[k * block : (k + 1) * block, :] = weights.astype(bf16)

    value_ref[...] = dot(weight_ref[...], rows_ref[...])
    for k in range(parts):
        columns = pl.ds(pl.multiple_of(k * (width // parts) + step * tile, tile), tile)
        value = value_ref[k * block : (k + 1) * block, :]
        if extra is not None:
            value = value + extra[:, columns].astype(f32)
        out_ref[:, columns] = value.astype(bf16)


def combined(index, home, share, rows, capacity, parts, extra=None, into=None, piece=0, pieces=1):
    slots, fold = rows.shape
    block = home.shape[0]
    width = parts * fold
    steps = 1
    placed = pl.BlockSpec((block, width), lambda i, q: (0, piece), pipeline_mode=pl.Buffered(1))
    ins = [
        whole(home.shape),
        whole(share.shape),
        pl.BlockSpec((slots, fold // steps), lambda i, q: (0, i)),
    ]
    args = [home, share, rows]
    if extra is not None:
        ins.append(placed)
        args.append(extra)
    if into is not None:
        ins.append(pl.BlockSpec(memory_space=pl.ANY))
        args.append(into)
    return pl.pallas_call(
        functools.partial(combine_body, capacity=capacity, parts=parts),
        out_shape=jax.ShapeDtypeStruct((block, width * pieces), bf16),
        grid_spec=pltpu.PrefetchScalarGridSpec(
            num_scalar_prefetch=1,
            grid=(steps,),
            in_specs=ins,
            out_specs=placed,
            scratch_shapes=[
                pltpu.VMEM((parts * block, slots), bf16),
                pltpu.VMEM((parts * block, fold // steps), f32),
            ],
        ),
        input_output_aliases={} if into is None else {len(args): 0},
        cost_estimate=pl.CostEstimate(
            flops=2 * parts * block * slots * fold,
            bytes_accessed=2 * slots * fold + 4 * block * width,
            transcendentals=0,
        ),
        compiler_params=limited("combined"),
        name="combined",
    )(index, *args)


def mixed_body(q_ref, hidden_ref, weight_ref, own_ref, *outs):
    step = pl.program_id(0)
    parts = 4
    block = own_ref.shape[0]
    middle = pl.num_programs(0) // 2

    def rows_for(which):
        start = pl.multiple_of((q_ref[0] + which) % parts * block, block)
        return dot(hidden_ref[pl.ds(start, block), :], weight_ref[...]).astype(bf16)

    own_ref[...] = rows_for(0)

    @pl.when(step < middle)
    def _():
        for k in range(parts - 1):
            outs[2 * k][...] = rows_for(k + 1)

    @pl.when(step >= middle)
    def _():
        for k in range(parts - 1):
            outs[2 * k + 1][...] = rows_for(k + 1)


def mixed_rows(index, hidden, weight, parts):
    rows, channels = hidden.shape
    width = weight.shape[1]
    steps = 4
    block, tile = rows // parts, width // steps
    low = pl.BlockSpec((block, tile), lambda i, q: (0, jnp.minimum(i, steps // 2 - 1)))
    high = pl.BlockSpec((block, tile), lambda i, q: (0, jnp.maximum(i - steps // 2, 0)))
    return call(
        mixed_body,
        "mixed_rows",
        (steps,),
        [whole(hidden.shape), pl.BlockSpec((channels, tile), lambda i, q: (0, i))],
        [((block, width), bf16, pl.BlockSpec((block, tile), lambda i, q: (0, i)))]
        + [((block, width // 2), bf16, low), ((block, width // 2), bf16, high)] * (parts - 1),
        (),
        2 * rows * channels * width,
        2 * (rows * channels + channels * width + rows * width),
    )(index, hidden, weight)


def on_device(
    mixer_value,
    mixer_gate,
    mixer_taps,
    mixer_gain,
    mixer_weight,
    routed_input,
    routed_gain,
    expert_ids,
    route_share,
    gate_weight,
    up_weight,
    down_weight,
):
    parts = lax.axis_size("tp")
    sources = lax.axis_size("ep")
    q = lax.axis_index("tp").astype(i32)
    index = q.reshape(1)
    across = (q + 2) % parts
    rows, width = routed_input.shape
    block = rows // parts
    capacity = 5 * block // (2 * sources)
    per_source = parts * capacity
    slots = sources * per_source
    quarter = width // parts
    side = 7 * quarter // 8
    early = 3 * slots // 4

    def exchanged(messages):
        size = messages.shape[1]
        messages = messages.reshape(sources, per_source, size)
        return lax.all_to_all(messages, "ep", 0, 0, tiled=True).reshape(slots, size)

    taps = mixer_taps.shape[0]
    length = mixer_value.shape[0]
    last_value, last_gate = mixer_value[length - (taps - 1) :], mixer_gate[length - (taps - 1) :]
    last = (last_value.astype(f32) * jax.nn.sigmoid(last_gate.astype(f32))).astype(bf16)
    before = lax.ppermute(last, "ep", [(i, i + 1) for i in range(sources - 1)])

    gain = routed_gain.reshape(-1, 128)
    near, factor, code = near_rows(
        index, expert_ids.T, routed_input, gain, slots, side, sources, capacity
    )
    near, before, mixer_value, mixer_gate, mixer_taps = lax.optimization_barrier(
        (near, before, mixer_value, mixer_gate, mixer_taps)
    )
    near = exchanged(near)
    gated = (mixer_value.astype(f32) * jax.nn.sigmoid(mixer_gate.astype(f32))).astype(bf16)

    extended = jnp.concatenate([before, gated], axis=0).astype(f32)
    taps_float = mixer_taps.astype(f32)
    filtered = taps_float[0] * extended[0:length]
    for offset in range(1, taps):
        filtered = filtered + taps_float[offset] * extended[offset : offset + length]
    stats = jnp.stack([jnp.sum(filtered, axis=1), jnp.sum(filtered * filtered, axis=1)])
    stats = stats + turned(stats, "tp", 1) + turned(stats, "tp", -1) + turned(stats, "tp", 2)
    channels = mixer_taps.shape[1] * parts
    center = stats[0] / channels
    spread = stats[1] / channels - center * center
    normed_mix = (
        (filtered - center[:, None])
        * lax.rsqrt(spread + 1e-05)[:, None]
        * mixer_gain.astype(f32)
    )
    mixer_hidden = jax.nn.silu(normed_mix).astype(bf16)
    mix_own, right_low, right_high, far_low, far_high, left_low, left_high = mixed_rows(
        index, mixer_hidden, mixer_weight, parts
    )
    via_right, via_left = turned(far_low, "tp", 1), turned(far_high, "tp", -1)
    raw_high, raw_low = turned(right_high, "tp", 1), turned(left_low, "tp", -1)

    factor, right_low, left_high = lax.optimization_barrier((factor, right_low, left_high))
    far = far_rows(index, code, routed_input, gain, factor, slots, side)
    lent = []
    for piece in (near[:early], near[early:]):
        lent.append((turned(piece, "tp", -1), turned(piece, "tp", 1)))
    far = exchanged(far)

    sum_low = turned((right_low.astype(f32) + via_right.astype(f32)).astype(bf16), "tp", 1)
    sum_high = turned((left_high.astype(f32) + via_left.astype(f32)).astype(bf16), "tp", -1)
    middle = width // 2
    mixer_result = jnp.concatenate(
        [
            mix_own[:, :middle].astype(f32) + sum_low.astype(f32) + raw_low.astype(f32),
            mix_own[:, middle:].astype(f32) + sum_high.astype(f32) + raw_high.astype(f32),
        ],
        axis=1,
    ).astype(bf16)

    weights = (gate_weight[0], up_weight[0])

    starts = first_part(index, near, *weights)
    sums = second_part(index, *lent[0], *starts, *weights)
    hidden = hidden_units(index, far, *lent[1], sums, starts, *weights, capacity)

    def home_of(which):
        own_code = lax.dynamic_slice_in_dim(code, which * block, block, 1) - which * capacity
        return own_code.T, lax.dynamic_slice_in_dim(route_share, which * block, block, 0)

    down = down_weight[0]
    far_home, own_home = home_of(across), home_of(q)
    got = []
    for piece in range(PIECES):
        to_right, to_left = side_rows(index, hidden, down, piece, PIECES)
        got.append((turned(to_right, "tp", 1), turned(to_left, "tp", -1)))
    messages = across_messages(index, hidden, down, capacity)
    far_back = exchanged(messages)
    own = [own_rows(index, hidden, down, piece, PIECES) for piece in range(PIECES)]
    extra = combined(index, *far_home, far_back, capacity, parts)
    extra, own[-1] = lax.optimization_barrier((extra, own[-1]))
    extra = turned(extra, "tp", 2)
    result = None
    for piece in range(PIECES):
        messages = summed_messages(index, own[piece], *got[piece], capacity, parts)
        back = exchanged(messages)
        result = combined(index, *own_home, back, capacity, parts, extra, result, piece, PIECES)
    return (mixer_result, result)


def solution(mesh):
    return jax.shard_map(
        on_device,
        mesh=mesh,
        in_specs=(
            P("ep", "tp"),
            P("ep", "tp"),
            P(None, "tp"),
            P("tp"),
            P("tp", None),
            P("ep", None),
            P(),
            P("ep", None),
            P("ep", None),
            P("ep", None, "tp"),
            P("ep", None, "tp"),
            P("ep", "tp", None),
        ),
        out_specs=(P(("ep", "tp"), None), P(("ep", "tp"), None)),
        check_vma=False,
    )
```
